32 devices in a mesh: kv: 8 (over z, y), tp: 4 (over x, core).
Axes of the slice: x: 2, y: 2, z: 4, core: 2. Of those that a mesh axis runs over, the one named last changes fastest.
Arguments:
- piece_tokens: bfloat16 [256, 2048], P('kv'), may hold values from -6 to 6
- decode_tokens: bfloat16 [16, 2048], P('kv'), may hold values from -6 to 6
- decode_lengths: int32 [16], P('kv'), may hold values from 1 to 2048, 16384 in all
- prompt_cache: bfloat16 [20480, 576], P('kv'), may hold values from -400 to 400
- decode_cache: bfloat16 [16, 2048, 576], P('kv'), may hold values from -400 to 400
- input_gain: float32 [2048], replicated, may hold values from 0.1 to 1.9
- query_down: bfloat16 [2048, 512], replicated, may hold values from -0.125 to 0.125
- query_gain: float32 [512], replicated, may hold values from 0.1 to 1.9
- query_nope_weight: bfloat16 [512, 2048], P(None, 'tp'), may hold values from -0.25 to 0.25
- query_rope_weight: bfloat16 [512, 1024], P(None, 'tp'), may hold values from -0.25 to 0.25
- latent_weight: bfloat16 [2048, 512], replicated, may hold values from -0.125 to 0.125
- latent_gain: float32 [512], replicated, may hold values from 0.1 to 1.9
- rotary_weight: bfloat16 [2048, 64], replicated, may hold values from -0.125 to 0.125
- key_up: bfloat16 [16, 128, 512], P('tp'), may hold values from -0.5 to 0.5
- value_up: bfloat16 [16, 512, 128], P('tp'), may hold values from -0.25 to 0.25
- out_weight: bfloat16 [2048, 2048], P('tp'), may hold values from -0.26516504 to 0.26516504
- out_gain: float32 [2048], P('tp'), may hold values from 0.1 to 1.9
Outputs:
- piece_out: float32 [256, 2048], P('kv', 'tp')
- decode_out: float32 [16, 2048], P('kv', 'tp')
- piece_keys: bfloat16 [256, 576], P('kv')
- decode_keys: bfloat16 [16, 576], P('kv')
The draws below stay inside these ranges and needn't reach their ends.
All inputs are finite; a program needn't handle non-finite values. No bound on the sum of `decode_lengths` on one device may be relied on, other than what follows from the above.
Results may differ from the reference program's by a relative error of at most 0.028.
The reference program's roundings to bfloat16 on the way count: a program that leaves them out, or rounds other values in their place, can miss the bound.
Values may be sent and summed in bfloat16 or wider, within the bound.
A program may use at most 128 MiB of HBM per device.

```python
import math
import jax
import jax.numpy as jnp
import numpy as np
from jax import lax

D = 2048
HEADS = 16
QRANK = 512
LATENT = 512
NOPE = 128
ROTARY = 64
VDIM = 128
CACHE_DEV = 2560
DEC_LEN = 2048
PIECE = 256
CACHE = 20480
DECODES = 16
N_KV = 8


def drawn_keys(key, row_count, width):
    base = jnp.clip(jax.random.normal(jax.random.fold_in(key, 11), (row_count, width), jnp.float32), -4.0, 4.0)
    return base


def draw_prompt_cache(key, part):
    return drawn_keys(key, CACHE, LATENT + ROTARY).astype(jnp.bfloat16)


def draw_decode_cache(key, part):
    flat = drawn_keys(key, DECODES * DEC_LEN, LATENT + ROTARY)
    return flat.reshape(DECODES, DEC_LEN, LATENT + ROTARY).astype(jnp.bfloat16)


def draw_out_weight(key, part):
    row_count = HEADS * VDIM
    base = jnp.clip(jax.random.normal(jax.random.fold_in(key, 21), (row_count, D), jnp.float32), -4.0, 4.0)
    base = base * row_count ** (-0.5)
    levels = jnp.array([0.35, 0.7, 1.4, 2.8], jnp.float32)
    ordering = jax.random.permutation(jax.random.fold_in(key, 22), 4)
    column_scale = levels[ordering][jnp.arange(D) // (D // 4)]
    return (base * column_scale[None, :]).astype(jnp.bfloat16)


def block_levels(own_key, dims, cuts, low, high):
    loudness = 1.0
    for axis_at, parts in cuts:
        draws = jax.random.uniform(jax.random.fold_in(jax.random.fold_in(own_key, 6), axis_at), (parts,), jnp.float32, low / len(cuts), high / len(cuts))
        loudness = loudness * jnp.repeat(jnp.exp(draws), dims[axis_at] // parts).reshape((-1,) + (1,) * (len(dims) - 1 - axis_at))
    return loudness


def split_up(number_of, total, most, slope):
    loads = [(1 << 20) // math.isqrt(grade ** slope) + 1 for grade in range(2, number_of + 1)]
    rest, holding = total - most - (number_of - 1), [1] * (number_of - 1)
    while rest > 0:
        movable = [i for i in range(number_of - 1) if holding[i] < most]
        whole, left = sum([loads[i] for i in movable]), rest
        for i in movable:
            more = min(most - holding[i], max(1, left * loads[i] // whole), rest)
            holding[i] = holding[i] + more
            rest = rest - more
    return np.array([most] + holding)


def ragged_sizes(key, number_of, total, bound, slope):
    if number_of == 2:
        one = jax.random.randint(key, (), max(1, total - bound), min(bound, total - 1) + 1)
        return jnp.stack([one, total - one])
    sizes = jnp.asarray(split_up(number_of, total, bound, slope), jnp.int32)
    twos = (number_of - 1) // 2
    donor, sink = sizes[1:1 + 2 * twos:2], sizes[2:2 + 2 * twos:2]
    slack = jnp.minimum(donor - 1, bound - sink)
    moved = jax.random.randint(jax.random.fold_in(key, 1), (twos,), 0, 1 << 20) % (slack + 1)
    sizes = sizes.at[1:1 + 2 * twos:2].set(donor - moved).at[2:2 + 2 * twos:2].set(sink + moved)
    return sizes[jax.random.permutation(jax.random.fold_in(key, 2), number_of)]


def noise(own_key, dims, scale, most, pieces=(), kind=jnp.bfloat16):
    entries = jax.random.normal(own_key, dims, jnp.float32) * scale
    if len(pieces) > 0:
        entries = block_levels(own_key, dims, pieces, -0.22, 0.18) * entries
    return jnp.clip(entries, min=-most, max=most).astype(kind)


def setup_inputs(seed: int = 0) -> dict:
    key_of = jax.random.split(jax.random.key(seed), 18)
    piece_tokens = noise(key_of[0], (PIECE, D), 1.0, 6.0, ((0, 8),))
    decode_tokens = noise(key_of[1], (DECODES, D), 1.0, 6.0, ((0, 8),))
    decode_lengths = ragged_sizes(key_of[2], DECODES, DECODES * DEC_LEN // 2, DEC_LEN, 0).astype(jnp.int32)
    prompt_cache = draw_prompt_cache(jax.random.fold_in(key_of[17], 71), 0)
    decode_cache = draw_decode_cache(jax.random.fold_in(key_of[17], 71), 0)
    input_gain = jnp.clip(1.0 + 0.18 * jax.random.normal(key_of[5], (D,), jnp.float32), 0.1, 1.9)
    query_down = noise(key_of[6], (D, QRANK), D ** -0.5, 0.125)
    query_gain = jnp.clip(1.0 + 0.18 * jax.random.normal(key_of[7], (QRANK,), jnp.float32), 0.1, 1.9)
    query_nope_weight = noise(key_of[8], (QRANK, HEADS * NOPE), QRANK ** -0.5, 0.25, ((1, 4),))
    query_rope_weight = noise(key_of[9], (QRANK, HEADS * ROTARY), QRANK ** -0.5, 0.25, ((1, 4),))
    latent_weight = noise(key_of[10], (D, LATENT), D ** -0.5, 0.125)
    latent_gain = jnp.clip(1.0 + 0.18 * jax.random.normal(key_of[11], (LATENT,), jnp.float32), 0.1, 1.9)
    rotary_weight = noise(key_of[12], (D, ROTARY), D ** -0.5, 0.125)
    key_up = noise(key_of[13], (HEADS, NOPE, LATENT), NOPE ** -0.5, 0.5, ((0, 4),))
    value_up = noise(key_of[14], (HEADS, LATENT, VDIM), LATENT ** -0.5, 0.25, ((0, 4),))
    out_weight = draw_out_weight(jax.random.fold_in(key_of[17], 71), 0)
    out_gain = jnp.clip(1.0 + 0.18 * jax.random.normal(key_of[16], (D,), jnp.float32), 0.1, 1.9)
    return {"piece_tokens": piece_tokens, "decode_tokens": decode_tokens, "decode_lengths": decode_lengths, "prompt_cache": prompt_cache, "decode_cache": decode_cache, "input_gain": input_gain, "query_down": query_down, "query_gain": query_gain, "query_nope_weight": query_nope_weight, "query_rope_weight": query_rope_weight, "latent_weight": latent_weight, "latent_gain": latent_gain, "rotary_weight": rotary_weight, "key_up": key_up, "value_up": value_up, "out_weight": out_weight, "out_gain": out_gain}


EPSILON = 1e-06
NEG_FILL = -1e+30
ROPE_BASE = 10000.0

def rounded(values):
    return lax.optimization_barrier(values.astype(jnp.bfloat16)).astype(jnp.float32)

def rms_scale(values, gain_vector):
    inverse = lax.rsqrt(lax.optimization_barrier(jnp.mean(values * values, axis=-1, keepdims=True)) + EPSILON)
    return values * inverse * gain_vector.astype(jnp.float32)

def rotate(values, positions):
    half_width = values.shape[-1] // 2
    inverse = ROPE_BASE ** (-jnp.arange(half_width, dtype=jnp.float32) / half_width)
    angles = positions.astype(jnp.float32)[:, None] * inverse[None, :]
    target = (angles.shape[0],) + (1,) * (values.ndim - 2) + (half_width,)
    cosine = jnp.cos(angles).reshape(target)
    sine_part = jnp.sin(angles).reshape(target)
    front_half = values[..., :half_width]
    back_half = values[..., half_width:]
    return jnp.concatenate([front_half * cosine - back_half * sine_part, back_half * cosine + front_half * sine_part], axis=-1)

def project(tokens, positions, input_gain, query_down, query_gain, query_nope_weight, query_rope_weight, latent_weight, latent_gain, rotary_weight, key_up):
    row_count = tokens.shape[0]
    head_count = key_up.shape[0]
    normed = rms_scale(tokens.astype(jnp.float32), input_gain).astype(jnp.bfloat16)
    compressed = rms_scale(jnp.dot(normed, query_down, preferred_element_type=jnp.float32), query_gain).astype(jnp.bfloat16)
    latent = rms_scale(jnp.dot(normed, latent_weight, preferred_element_type=jnp.float32), latent_gain).astype(jnp.bfloat16)
    rotary = rotate(jnp.dot(normed, rotary_weight, preferred_element_type=jnp.float32), positions).astype(jnp.bfloat16)
    new_keys = jnp.concatenate([latent, rotary], axis=-1)
    query_nope = jnp.dot(compressed, query_nope_weight, preferred_element_type=jnp.float32).astype(jnp.bfloat16)
    query_nope = query_nope.reshape(row_count, head_count, -1)
    query_rope = jnp.dot(compressed, query_rope_weight, preferred_element_type=jnp.float32).reshape(row_count, head_count, -1)
    query_rope = rotate(query_rope, positions).astype(jnp.bfloat16)
    absorbed = jnp.einsum('thn,hnr->thr', query_nope.astype(jnp.float32), key_up.astype(jnp.float32)).astype(jnp.bfloat16)
    return (new_keys, jnp.concatenate([absorbed, query_rope], axis=-1))

def reference(piece_tokens, decode_tokens, decode_lengths, prompt_cache, decode_cache, input_gain, query_down, query_gain, query_nope_weight, query_rope_weight, latent_weight, latent_gain, rotary_weight, key_up, value_up, out_weight, out_gain):
    score_scale = (NOPE + ROTARY) ** (-0.5)
    piece_index = jnp.arange(PIECE, dtype=jnp.int32)
    positions = jnp.concatenate([CACHE + piece_index, decode_lengths.astype(jnp.int32)])
    tokens = jnp.concatenate([piece_tokens, decode_tokens], axis=0)
    new_keys, queries = project(tokens, positions, input_gain, query_down, query_gain, query_nope_weight, query_rope_weight, latent_weight, latent_gain, rotary_weight, key_up)
    piece_keys = new_keys[:PIECE]
    decode_keys = new_keys[PIECE:]
    piece_queries = queries[:PIECE].astype(jnp.float32)
    decode_queries = queries[PIECE:].astype(jnp.float32)
    causal = (piece_index[None, :] <= piece_index[:, None])[:, None, :]
    own_scores = jnp.einsum('thc,kc->thk', piece_queries, piece_keys.astype(jnp.float32)) * score_scale
    own_scores = jnp.where(causal, own_scores, NEG_FILL)
    own_max = lax.optimization_barrier(jnp.max(own_scores, axis=-1))
    own_weights = jnp.where(causal, jnp.exp(own_scores - own_max[..., None]), 0.0)
    own_sum = lax.optimization_barrier(jnp.sum(own_weights, axis=-1))
    own_values = jnp.einsum('thk,kr->thr', rounded(own_weights), piece_keys[:, :LATENT].astype(jnp.float32))

    def one_shard(running, shard):
        best_max, total_sum, weighted = running
        shard_data = shard.astype(jnp.float32)
        scores = jnp.einsum('thc,kc->thk', piece_queries, shard_data) * score_scale
        shard_max = lax.optimization_barrier(jnp.max(scores, axis=-1))
        weights = jnp.exp(scores - shard_max[..., None])
        shard_sum = lax.optimization_barrier(jnp.sum(weights, axis=-1))
        shard_values = rounded(jnp.einsum('thk,kr->thr', rounded(weights), shard_data[:, :LATENT]))
        new_best = jnp.maximum(best_max, shard_max)
        keep_old = jnp.exp(best_max - new_best)
        take_new = jnp.exp(shard_max - new_best)
        return ((new_best, total_sum * keep_old + shard_sum * take_new, weighted * keep_old[..., None] + shard_values * take_new[..., None]), None)
    initial = (jnp.full((PIECE, HEADS), NEG_FILL, jnp.float32), jnp.zeros((PIECE, HEADS), jnp.float32), jnp.zeros((PIECE, HEADS, LATENT), jnp.float32))
    finals, unused = lax.scan(one_shard, initial, prompt_cache.reshape(N_KV, CACHE_DEV, LATENT + ROTARY))
    cache_max, cache_sum, cache_values = finals
    joint_max = jnp.maximum(cache_max, own_max)
    cache_factor = jnp.exp(cache_max - joint_max)
    own_factor = jnp.exp(own_max - joint_max)
    numerator = cache_values * cache_factor[..., None] + own_values * own_factor[..., None]
    denominator = cache_sum * cache_factor + own_sum * own_factor
    piece_latent = numerator / denominator[..., None]
    slot_index = jnp.arange(DEC_LEN, dtype=jnp.int32)
    live_slots = (slot_index[None, :] < decode_lengths.astype(jnp.int32)[:, None])[:, None, :]
    past_scores = jnp.einsum('bhc,bkc->bhk', decode_queries, decode_cache.astype(jnp.float32)) * score_scale
    past_scores = jnp.where(live_slots, past_scores, NEG_FILL)
    self_scores = jnp.einsum('bhc,bc->bh', decode_queries, decode_keys.astype(jnp.float32)) * score_scale
    decode_max = jnp.maximum(lax.optimization_barrier(jnp.max(past_scores, axis=-1)), self_scores)
    past_weights = jnp.where(live_slots, jnp.exp(past_scores - decode_max[..., None]), 0.0)
    self_weights = jnp.exp(self_scores - decode_max)
    decode_sum = lax.optimization_barrier(jnp.sum(past_weights, axis=-1)) + self_weights
    decode_values = jnp.einsum('bhk,bkr->bhr', rounded(past_weights), decode_cache[:, :, :LATENT].astype(jnp.float32))
    decode_values = decode_values + rounded(self_weights)[..., None] * decode_keys[:, None, :LATENT].astype(jnp.float32)
    decode_latent = decode_values / decode_sum[..., None]
    latents = jnp.concatenate([piece_latent, decode_latent], axis=0)
    head_out = jnp.einsum('thr,hrv->thv', latents, value_up.astype(jnp.float32), precision=lax.Precision.HIGHEST).astype(jnp.bfloat16)
    head_out = head_out.reshape(head_out.shape[0], -1)
    mixture = jnp.dot(head_out, out_weight, preferred_element_type=jnp.float32)
    result = rms_scale(mixture, out_gain)
    return (result[:PIECE], result[PIECE:], piece_keys, decode_keys)
```

```python
import functools

import jax
import jax.numpy as jnp
from jax import lax
from jax.experimental import pallas as pl
from jax.experimental.pallas import tpu as pltpu
from jax.sharding import PartitionSpec as P

EPSILON = 1e-06
NEG_FILL = -1e30
ROPE_BASE = 10000.0
MESH = pl.DeviceIdType.MESH
F32 = jnp.float32
BF16 = jnp.bfloat16


def dot(a, b):
    return jnp.dot(a, b, preferred_element_type=F32)


def dot_t(a, b):
    return lax.dot_general(a, b, (((1,), (1,)), ((), ())), preferred_element_type=F32)


def dot_wide(a, b):
    high = a.astype(BF16)
    low = (a - high.astype(F32)).astype(BF16)
    return dot(high, b) + dot(low, b)


def rms(x, gain):
    return x * lax.rsqrt(jnp.mean(x * x, axis=-1, keepdims=True) + EPSILON) * gain


def lanes(shape):
    return lax.broadcasted_iota(jnp.int32, shape, len(shape) - 1)


def swap_halves(x, rotary):
    width = x.shape[-1]
    half = rotary // 2
    first = lax.rem(lanes(x.shape), rotary) < half
    return jnp.where(first, pltpu.roll(x, width - half, 1), pltpu.roll(x, half, 1))


def kernel(n_kv, n_tp, pair, names, *refs):
    r = dict(zip(names, refs))
    kv = lax.axis_index("kv")
    tp = lax.axis_index("tp")
    loads = (
        "piece", "decode", "input_gain", "down", "query_gain", "latent", "latent_gain",
        "rotary", "cos", "sin", "nope", "rope", "key_up", "dcache", "pcache", "value_up",
        "out_w", "out_gain",
    )
    local = {
        name: pltpu.make_async_copy(r[name + "_hbm"], r[name], r["load_sem"].at[i])
        for i, name in enumerate(loads)
    }
    for name in loads:
        local[name].start()
    barrier = pltpu.get_barrier_semaphore()
    for d in range(1, n_kv):
        pl.semaphore_signal(
            barrier, inc=1, device_id={"kv": lax.rem(kv + d, n_kv)}, device_id_type=MESH
        )
    for d in range(1, n_tp):
        pl.semaphore_signal(
            barrier, inc=1, device_id={"tp": lax.rem(tp + d, n_tp)}, device_id_type=MESH
        )

    rows = r["piece"].shape[0]
    decodes = r["decode"].shape[0]
    extra = r["tok"].shape[0] - rows
    total = rows + extra
    lat = r["latent"].shape[1]
    qrank = r["down"].shape[1]
    rot = r["rotary"].shape[1]
    heads, nope_w = r["key_up"].shape[0], r["key_up"].shape[1]
    vdim = r["value_up"].shape[2]
    scale = (nope_w + rot) ** (-0.5)
    gath = r["gath"]
    wide = gath.shape[2] - qrank - lat

    tok = r["tok"]
    local["piece"].wait()
    local["decode"].wait()
    local["input_gain"].wait()
    tok[0:rows, :] = r["piece"][...].astype(F32)
    tok[rows:total, :] = jnp.zeros((extra, tok.shape[1]), F32)
    tok[rows : rows + decodes, :] = r["decode"][...].astype(F32)
    normed = rms(tok[...], r["input_gain"][...]).astype(BF16)
    local["down"].wait()
    local["query_gain"].wait()
    comp = rms(dot(normed, r["down"][...]), r["query_gain"][...]).astype(BF16)
    local["latent"].wait()
    local["latent_gain"].wait()
    latent = rms(dot(normed, r["latent"][...]), r["latent_gain"][...]).astype(BF16)
    local["rotary"].wait()
    local["cos"].wait()
    local["sin"].wait()
    rk = r["rk"]
    rk[...] = jnp.zeros(rk.shape, F32)
    rk[:, 0:rot] = dot(normed, r["rotary"][...])
    piece_total = n_kv * rows
    own_rows = pl.ds(pl.multiple_of(kv * rows, rows), rows)
    tab = r["tab"]
    tab[0, 0:rows, :] = r["cos"][own_rows, :]
    tab[0, rows:total, :] = r["cos"][piece_total : piece_total + extra, :]
    tab[1, 0:rows, :] = r["sin"][own_rows, :]
    tab[1, rows:total, :] = r["sin"][piece_total : piece_total + extra, :]
    raw = rk[...]
    rotary = (raw * tab[0, :, 0 : rk.shape[1]] + swap_halves(raw, rot) * tab[1, :, 0 : rk.shape[1]]).astype(BF16)
    gath[kv, :, 0:qrank] = comp[0:rows]
    gath[kv, :, qrank : qrank + lat] = latent[0:rows]
    gath[kv, :, qrank + lat :] = rotary[0:rows, 0:wide]

    def gather_copy(slot, peer, d):
        return pltpu.make_async_remote_copy(
            src_ref=gath.at[slot], dst_ref=gath.at[slot],
            send_sem=r["g_send"].at[d], recv_sem=r["g_recv"].at[slot],
            device_id={"kv": peer}, device_id_type=MESH,
        )

    pl.semaphore_wait(barrier, n_kv - 1 + n_tp - 1)
    for d in range(1, n_kv):
        gather_copy(kv, lax.rem(kv + d, n_kv), d).start()

    r["piece_keys"][:, 0:lat] = latent[0:rows]
    r["piece_keys"][:, lat:] = rotary[0:rows, 0:rot]
    r["decode_keys"][:, 0:lat] = latent[rows : rows + decodes]
    r["decode_keys"][:, lat:] = rotary[rows : rows + decodes, 0:rot]

    local["nope"].wait()
    local["rope"].wait()
    local["key_up"].wait()

    def make_queries(comp_rows, cosine, sine, q_ref):
        t = comp_rows.shape[0]
        qn = dot(comp_rows, r["nope"][...]).astype(BF16)
        qr = dot(comp_rows, r["rope"][...])
        width = qr.shape[1]
        reps = width // cosine.shape[1]
        cosine = jnp.concatenate([cosine] * reps, axis=1)
        sine = jnp.concatenate([sine] * reps, axis=1)
        qr = qr * cosine + swap_halves(qr, rot) * sine
        for h in range(heads):
            q_ref[h * t : (h + 1) * t, 0:lat] = dot(
                qn[:, h * nope_w : (h + 1) * nope_w], r["key_up"][h]
            ).astype(BF16)
            shift = (width - h * rot) % width
            part = pltpu.roll(qr, shift, 1) if shift else qr
            q_ref[h * t : (h + 1) * t, lat:] = part[:, 0:rot].astype(BF16)

    qo = r["qo"]
    make_queries(comp, tab[0], tab[1], qo)
    dq = jnp.concatenate([qo[h * total + rows : (h + 1) * total, :] for h in range(heads)], axis=0)
    drows = heads * extra

    local["dcache"].wait()
    dkeys_lat = latent[rows:total].astype(F32)
    dkeys_rot = rotary[rows:total, 0:rot].astype(F32)
    tiled_lat = jnp.concatenate([dkeys_lat] * heads, axis=0)
    tiled_rot = jnp.concatenate([dkeys_rot] * heads, axis=0)
    self_score = (
        jnp.sum(dq[:, 0:lat].astype(F32) * tiled_lat, axis=-1, keepdims=True)
        + jnp.sum(dq[:, lat:].astype(F32) * tiled_rot, axis=-1, keepdims=True)
    ) * scale
    row_of = lax.rem(lax.broadcasted_iota(jnp.int32, (drows, lat), 0), extra)
    dlat = jnp.zeros((drows, lat), F32)
    slots = r["dcache"].shape[1]
    for b in range(decodes):
        s = dot_t(dq[:, 0:lat], r["dcache"][b, :, 0:lat]) + dot_t(dq[:, lat:], r["dcache"][b, :, lat:])
        live = lanes((drows, slots)) < r["lengths"][b]
        s = jnp.where(live, s * scale, NEG_FILL)
        m = jnp.maximum(jnp.max(s, axis=-1, keepdims=True), self_score)
        w = jnp.where(live, jnp.exp(s - m), 0.0)
        w_self = jnp.exp(self_score - m)
        norm = jnp.sum(w, axis=-1, keepdims=True) + w_self
        v = dot(w.astype(BF16), r["dcache"][b, :, 0:lat])
        v = (v + w_self.astype(BF16).astype(F32) * tiled_lat) / norm
        dlat = jnp.where(row_of == b, v, dlat)
    local["value_up"].wait()
    ho = r["ho"]
    for h in range(heads):
        ho[rows:total, h * vdim : (h + 1) * vdim] = dot_wide(
            dlat[h * extra : (h + 1) * extra], r["value_up"][h]
        ).astype(BF16)

    local["pcache"].wait()
    sendv, recvv, sends, recvs = r["sendv"], r["recvv"], r["sends"], r["recvs"]
    chunk = pair * rows
    qc = r["qc"]

    def value_copy(mine, peer):
        return pltpu.make_async_remote_copy(
            src_ref=sendv.at[peer], dst_ref=recvv.at[mine],
            send_sem=r["v_send"].at[peer], recv_sem=r["v_recv"].at[mine],
            device_id={"kv": peer}, device_id_type=MESH,
        )

    def stat_copy(mine, peer):
        return pltpu.make_async_remote_copy(
            src_ref=sends.at[peer], dst_ref=recvs.at[mine],
            send_sem=r["s_send"].at[peer], recv_sem=r["s_recv"].at[mine],
            device_id={"kv": peer}, device_id_type=MESH,
        )

    stat_lane = lanes((rows, 128))

    def stats(m, norm, t, start):
        out = jnp.zeros((rows, 128), F32)
        for h in range(heads):
            at = h * t + start
            out = jnp.where(stat_lane == h, m[at : at + rows], out)
            out = jnp.where(stat_lane == heads + h, norm[at : at + rows], out)
        return out

    def chunk_step(c, carry):
        base = lax.rem(lax.div(kv, pair) + c, n_kv // pair) * pair
        for i in range(pair):
            @pl.when(base + i != kv)
            def _():
                gather_copy(base + i, kv, 0).wait_recv()
        at = pl.ds(pl.multiple_of(base * rows, chunk), chunk)
        comp_rows = gath[pl.ds(base, pair), :, 0:qrank].reshape(chunk, qrank)
        make_queries(comp_rows, r["cos"][at, :], r["sin"][at, :], qc)
        s = (
            dot_t(qc[:, 0:lat], r["pcache"][:, 0:lat]) + dot_t(qc[:, lat:], r["pcache"][:, lat:])
        ) * scale
        m = jnp.max(s, axis=-1, keepdims=True)
        w = jnp.exp(s - m)
        norm = jnp.sum(w, axis=-1, keepdims=True)
        v = dot(w.astype(BF16), r["pcache"][:, 0:lat]).astype(BF16)
        for h in range(heads):
            pv = dot(v[h * chunk : (h + 1) * chunk], r["value_up"][h]).astype(BF16)
            for i in range(pair):
                sendv[base + i, :, h * vdim : (h + 1) * vdim] = pv[i * rows : (i + 1) * rows]
        for i in range(pair):
            sends[base + i] = stats(m, norm, chunk, i * rows)
        for i in range(pair):
            @pl.when(base + i != kv)
            def _():
                value_copy(kv, base + i).start()
                stat_copy(kv, base + i).start()
        return carry

    lax.fori_loop(0, n_kv // pair, chunk_step, 0)

    own_q = jnp.concatenate([qo[h * total : h * total + rows, :] for h in range(heads)], axis=0)
    every = gath[...].reshape(piece_total, gath.shape[2])
    key_lat = every[:, qrank : qrank + lat]
    s = dot_t(own_q[:, 0:lat], key_lat) + dot_t(own_q[:, lat:], every[:, qrank + lat : qrank + lat + rot])
    row = lax.rem(lax.broadcasted_iota(jnp.int32, s.shape, 0), rows) + kv * rows
    causal = lanes(s.shape) <= row
    s = jnp.where(causal, s * scale, NEG_FILL)
    m = jnp.max(s, axis=-1, keepdims=True)
    w = jnp.where(causal, jnp.exp(s - m), 0.0)
    norm = jnp.sum(w, axis=-1, keepdims=True)
    own_v = dot(w.astype(BF16), key_lat)
    own_stats = stats(m, norm, rows, 0)
    own_p = [dot_wide(own_v[h * rows : (h + 1) * rows], r["value_up"][h]) for h in range(heads)]

    recvv[kv] = sendv[kv]
    recvs[kv] = sends[kv]
    for d in range(1, n_kv):
        peer = lax.rem(kv + n_kv - d, n_kv)
        stat_copy(peer, kv).wait_recv()
        value_copy(peer, kv).wait_recv()
    joint = own_stats
    for j in range(n_kv):
        joint = jnp.maximum(joint, recvs[j])
    factor = jnp.exp(own_stats - joint)
    bottom = pltpu.roll(own_stats, 128 - heads, 1) * factor
    top = [own_p[h] * factor[:, h : h + 1] for h in range(heads)]
    for j in range(n_kv):
        st = recvs[j]
        factor = jnp.exp(st - joint)
        bottom = bottom + pltpu.roll(st, 128 - heads, 1) * factor
        for h in range(heads):
            top[h] = top[h] + recvv[j, :, h * vdim : (h + 1) * vdim].astype(F32) * factor[:, h : h + 1]
    for h in range(heads):
        ho[0:rows, h * vdim : (h + 1) * vdim] = (top[h] / bottom[:, h : h + 1]).astype(BF16)

    local["out_w"].wait()
    local["out_gain"].wait()
    mixs, mixr, sqs, sqr = r["mixs"], r["mixr"], r["sqs"], r["sqr"]
    cols = mixs.shape[2]

    def mix_copy(mine, peer):
        return pltpu.make_async_remote_copy(
            src_ref=mixs.at[peer], dst_ref=mixr.at[mine],
            send_sem=r["m_send"].at[peer], recv_sem=r["m_recv"].at[mine],
            device_id={"tp": peer}, device_id_type=MESH,
        )

    def square_copy(mine, peer):
        return pltpu.make_async_remote_copy(
            src_ref=sqs, dst_ref=sqr.at[mine],
            send_sem=r["q_send"].at[peer], recv_sem=r["q_recv"].at[mine],
            device_id={"tp": peer}, device_id_type=MESH,
        )

    head_out = ho[...]
    for d in range(1, n_tp):
        peer = lax.rem(tp + d, n_tp)
        at = pl.ds(pl.multiple_of(peer * cols, 128), cols)
        mixs[peer] = dot(head_out, r["out_w"][:, at]).astype(BF16)
        mix_copy(tp, peer).start()
    mix = dot(head_out, r["out_w"][:, pl.ds(pl.multiple_of(tp * cols, 128), cols)])
    for d in range(1, n_tp):
        peer = lax.rem(tp + n_tp - d, n_tp)
        mix_copy(peer, tp).wait_recv()
        mix = mix + mixr[peer].astype(F32)
    squares = jnp.sum(mix * mix, axis=-1, keepdims=True)
    sqs[...] = jnp.broadcast_to(squares, sqs.shape)
    for d in range(1, n_tp):
        square_copy(tp, lax.rem(tp + d, n_tp)).start()
    for d in range(1, n_tp):
        peer = lax.rem(tp + n_tp - d, n_tp)
        square_copy(peer, tp).wait_recv()
        squares = squares + sqr[peer][:, 0:1]
    result = mix * lax.rsqrt(squares / (cols * n_tp) + EPSILON) * r["out_gain"][...]
    r["piece_out"][...] = result[0:rows]
    r["decode_out"][...] = result[rows : rows + decodes]

    for d in range(1, n_kv):
        peer = lax.rem(kv + d, n_kv)
        gather_copy(kv, peer, d).wait_send()
        value_copy(kv, peer).wait_send()
        stat_copy(kv, peer).wait_send()
    for d in range(1, n_tp):
        peer = lax.rem(tp + d, n_tp)
        mix_copy(tp, peer).wait_send()
        square_copy(tp, peer).wait_send()


def shards(
    n_kv, n_tp,
    piece_tokens, decode_tokens, decode_lengths, prompt_cache, decode_cache, input_gain,
    query_down, query_gain, query_nope_weight, query_rope_weight, latent_weight, latent_gain,
    rotary_weight, key_up, value_up, out_weight, out_gain,
):
    rows, model = piece_tokens.shape
    decodes = decode_tokens.shape[0]
    extra = -(-decodes // 16) * 16
    total = rows + extra
    heads = key_up.shape[0]
    lat = latent_gain.shape[0]
    qrank = query_gain.shape[0]
    rot = rotary_weight.shape[1]
    half = rot // 2
    piece_total = rows * n_kv
    positions = jnp.concatenate(
        [
            prompt_cache.shape[0] * n_kv + jnp.arange(piece_total, dtype=jnp.int32),
            decode_lengths,
            jnp.zeros((extra - decodes,), jnp.int32),
        ]
    )
    lane = jnp.arange(128, dtype=jnp.int32)
    inverse = ROPE_BASE ** (-(lane % half).astype(F32) / half)
    angles = positions.astype(F32)[:, None] * inverse[None, :]
    cosine = jnp.cos(angles)
    sine = jnp.sin(angles) * jnp.where(lane % rot < half, -1.0, 1.0)[None, :]
    pair = 2 if n_kv % 2 == 0 else 1
    wide = -(-rot // 128) * 128
    cols = out_gain.shape[0]

    args = {
        "lengths": decode_lengths,
        "piece": piece_tokens, "decode": decode_tokens, "input_gain": input_gain[None],
        "down": query_down, "query_gain": query_gain[None], "latent": latent_weight,
        "latent_gain": latent_gain[None], "rotary": rotary_weight, "cos": cosine, "sin": sine,
        "nope": query_nope_weight, "rope": query_rope_weight, "key_up": key_up,
        "dcache": decode_cache, "pcache": prompt_cache, "value_up": value_up,
        "out_w": out_weight, "out_gain": out_gain[None],
    }
    outs = {
        "piece_out": ((rows, cols), F32), "decode_out": ((decodes, cols), F32),
        "piece_keys": ((rows, lat + rot), BF16), "decode_keys": ((decodes, lat + rot), BF16),
    }
    width = lat + rot
    vdim = value_up.shape[2]
    scratch = {k: pltpu.VMEM(v.shape, v.dtype) for k, v in args.items() if k != "lengths"}
    scratch |= {
        "tok": pltpu.VMEM((total, model), F32),
        "rk": pltpu.VMEM((total, 128), F32),
        "tab": pltpu.VMEM((2, total, 128), F32),
        "gath": pltpu.VMEM((n_kv, rows, qrank + lat + wide), BF16),
        "qo": pltpu.VMEM((heads * total, width), BF16),
        "qc": pltpu.VMEM((heads * pair * rows, width), BF16),
        "ho": pltpu.VMEM((total, heads * vdim), BF16),
        "sendv": pltpu.VMEM((n_kv, rows, heads * vdim), BF16),
        "recvv": pltpu.VMEM((n_kv, rows, heads * vdim), BF16),
        "sends": pltpu.VMEM((n_kv, rows, 128), F32),
        "recvs": pltpu.VMEM((n_kv, rows, 128), F32),
        "mixs": pltpu.VMEM((n_tp, total, cols), BF16),
        "mixr": pltpu.VMEM((n_tp, total, cols), BF16),
        "sqs": pltpu.VMEM((total, 128), F32),
        "sqr": pltpu.VMEM((n_tp, total, 128), F32),
        "load_sem": pltpu.SemaphoreType.DMA((len(args) - 1,)),
    }
    for k in ("g", "v", "s"):
        scratch[k + "_send"] = pltpu.SemaphoreType.DMA((n_kv,))
        scratch[k + "_recv"] = pltpu.SemaphoreType.DMA((n_kv,))
    for k in ("m", "q"):
        scratch[k + "_send"] = pltpu.SemaphoreType.DMA((n_tp,))
        scratch[k + "_recv"] = pltpu.SemaphoreType.DMA((n_tp,))
    names = [k if k == "lengths" else k + "_hbm" for k in args] + list(outs) + list(scratch)
    return pl.pallas_call(
        functools.partial(kernel, n_kv, n_tp, pair, names),
        out_shape=[jax.ShapeDtypeStruct(*v) for v in outs.values()],
        in_specs=[
            pl.BlockSpec(memory_space=pltpu.SMEM if k == "lengths" else pl.ANY) for k in args
        ],
        out_specs=[pl.BlockSpec(memory_space=pltpu.VMEM) for _ in outs],
        scratch_shapes=list(scratch.values()),
        compiler_params=pltpu.CompilerParams(
            collective_id=0, has_side_effects=True, vmem_limit_bytes=60000 * 1024
        ),
    )(*args.values())


def solution(mesh):
    in_specs = (
        P("kv", None), P("kv", None), P("kv"), P("kv", None), P("kv", None, None), P(), P(), P(),
        P(None, "tp"), P(None, "tp"), P(), P(), P(), P("tp", None, None), P("tp", None, None),
        P("tp", None), P("tp"),
    )
    out_specs = (P("kv", "tp"), P("kv", "tp"), P("kv", None), P("kv", None))
    body = functools.partial(shards, mesh.shape["kv"], mesh.shape["tp"])
    return jax.shard_map(
        body, mesh=mesh, in_specs=in_specs, out_specs=out_specs, check_vma=False
    )
```

```python
import functools

import jax
import jax.numpy as jnp
from jax import lax
from jax.experimental import pallas as pl
from jax.experimental.pallas import tpu as pltpu
from jax.sharding import PartitionSpec as P

EPSILON = 1e-06
NEG_FILL = -1e30
ROPE_BASE = 10000.0
MESH = pl.DeviceIdType.MESH
F32 = jnp.float32
BF16 = jnp.bfloat16


def dot(a, b):
    return jnp.dot(a, b, preferred_element_type=F32)


def dot_t(a, b):
    return lax.dot_general(a, b, (((1,), (1,)), ((), ())), preferred_element_type=F32)


def dot_wide(a, b):
    high = a.astype(BF16)
    low = (a - high.astype(F32)).astype(BF16)
    return dot(high, b) + dot(low, b)


def rms(x, gain):
    return x * lax.rsqrt(jnp.mean(x * x, axis=-1, keepdims=True) + EPSILON) * gain


def lanes(shape):
    return lax.broadcasted_iota(jnp.int32, shape, len(shape) - 1)


def swap_halves(x, rotary):
    width = x.shape[-1]
    half = rotary // 2
    first = lax.rem(lanes(x.shape), rotary) < half
    return jnp.where(first, pltpu.roll(x, width - half, 1), pltpu.roll(x, half, 1))


def kernel(n_kv, n_tp, pair, names, *refs):
    r = dict(zip(names, refs))
    kv = lax.axis_index("kv")
    tp = lax.axis_index("tp")
    loads = (
        "piece", "decode", "input_gain", "down", "query_gain", "latent", "latent_gain",
        "rotary", "nope", "rope", "key_up", "dcache", "pcache", "value_up",
        "out_w", "out_gain",
    )
    local = {
        name: pltpu.make_async_copy(r[name + "_hbm"], r[name], r["load_sem"].at[i])
        for i, name in enumerate(loads)
    }
    for name in loads:
        local[name].start()
    barrier = pltpu.get_barrier_semaphore()
    for d in range(1, n_kv):
        pl.semaphore_signal(
            barrier, inc=1, device_id={"kv": lax.rem(kv + d, n_kv)}, device_id_type=MESH
        )
    for d in range(1, n_tp):
        pl.semaphore_signal(
            barrier, inc=1, device_id={"tp": lax.rem(tp + d, n_tp)}, device_id_type=MESH
        )

    rows = r["piece"].shape[0]
    decodes = r["decode"].shape[0]
    extra = r["tok"].shape[0] - rows
    total = rows + extra
    lat = r["latent"].shape[1]
    qrank = r["down"].shape[1]
    rot = r["rotary"].shape[0]
    heads, nope_w = r["key_up"].shape[0], r["key_up"].shape[1]
    vdim = r["value_up"].shape[2]
    scale = (nope_w + rot) ** (-0.5)
    gath = r["gath"]
    wide = gath.shape[2] - qrank - lat

    piece_total = n_kv * rows
    shape = r["cos"].shape
    row_at = lax.broadcasted_iota(jnp.int32, shape, 0)
    position = row_at + r["pcache"].shape[1] * n_kv
    for b in range(decodes):
        position = jnp.where(row_at == piece_total + b, r["lengths"][b], position)
    lane = lanes((1, shape[1]))
    inverse = ROPE_BASE ** (-lax.rem(lane, rot // 2).astype(F32) / (rot // 2))
    angle = position.astype(F32) * inverse
    r["cos"][...] = jnp.cos(angle)
    sine = jnp.sin(angle)
    r["sin"][...] = jnp.where(lax.rem(lanes(shape), rot) < rot // 2, -sine, sine)

    tok = r["tok"]
    local["piece"].wait()
    local["decode"].wait()
    local["input_gain"].wait()
    tok[0:rows, :] = r["piece"][...].astype(F32)
    tok[rows:total, :] = jnp.zeros((extra, tok.shape[1]), F32)
    tok[rows : rows + decodes, :] = r["decode"][...].astype(F32)
    normed = rms(tok[...], r["input_gain"][...]).astype(BF16)
    local["down"].wait()
    local["query_gain"].wait()
    comp = rms(dot(normed, r["down"][...]), r["query_gain"][...]).astype(BF16)
    local["latent"].wait()
    local["latent_gain"].wait()
    latent = rms(dot(normed, r["latent"][...]), r["latent_gain"][...]).astype(BF16)
    local["rotary"].wait()
    rk = r["rk"]
    rk[...] = jnp.zeros(rk.shape, F32)
    rk[:, 0:rot] = dot_t(normed, r["rotary"][...])
    own_rows = pl.ds(pl.multiple_of(kv * rows, rows), rows)
    tab = r["tab"]
    tab[0, 0:rows, :] = r["cos"][own_rows, :]
    tab[0, rows:total, :] = r["cos"][piece_total : piece_total + extra, :]
    tab[1, 0:rows, :] = r["sin"][own_rows, :]
    tab[1, rows:total, :] = r["sin"][piece_total : piece_total + extra, :]
    raw = rk[...]
    rotary = (raw * tab[0, :, 0 : rk.shape[1]] + swap_halves(raw, rot) * tab[1, :, 0 : rk.shape[1]]).astype(BF16)
    gath[kv, :, 0:qrank] = comp[0:rows]
    gath[kv, :, qrank : qrank + lat] = latent[0:rows]
    gath[kv, :, qrank + lat :] = rotary[0:rows, 0:wide]

    def gather_copy(slot, peer, d):
        return pltpu.make_async_remote_copy(
            src_ref=gath.at[slot], dst_ref=gath.at[slot],
            send_sem=r["g_send"].at[d], recv_sem=r["g_recv"].at[slot],
            device_id={"kv": peer}, device_id_type=MESH,
        )

    pl.semaphore_wait(barrier, n_kv - 1 + n_tp - 1)
    for d in range(1, n_kv):
        gather_copy(kv, lax.rem(kv + d, n_kv), d).start()

    r["piece_keys"][:, 0:lat] = latent[0:rows]
    r["piece_keys"][:, lat:] = rotary[0:rows, 0:rot]
    r["decode_keys"][:, 0:lat] = latent[rows : rows + decodes]
    r["decode_keys"][:, lat:] = rotary[rows : rows + decodes, 0:rot]

    local["nope"].wait()
    local["rope"].wait()
    local["key_up"].wait()

    def make_queries(comp_rows, cosine, sine, q_ref):
        t = comp_rows.shape[0]
        qn = dot(comp_rows, r["nope"][...]).astype(BF16)
        qr = dot(comp_rows, r["rope"][...])
        width = qr.shape[1]
        reps = width // cosine.shape[1]
        cosine = jnp.concatenate([cosine] * reps, axis=1)
        sine = jnp.concatenate([sine] * reps, axis=1)
        qr = qr * cosine + swap_halves(qr, rot) * sine
        for h in range(heads):
            q_ref[h * t : (h + 1) * t, 0:lat] = dot(
                qn[:, h * nope_w : (h + 1) * nope_w], r["key_up"][h]
            ).astype(BF16)
            shift = (width - h * rot) % width
            part = pltpu.roll(qr, shift, 1) if shift else qr
            q_ref[h * t : (h + 1) * t, lat:] = part[:, 0:rot].astype(BF16)

    qo = r["qo"]
    make_queries(comp, tab[0], tab[1], qo)
    dq = jnp.concatenate([qo[h * total + rows : (h + 1) * total, :] for h in range(heads)], axis=0)
    drows = heads * extra

    local["dcache"].wait()
    dkeys_lat = latent[rows:total].astype(F32)
    dkeys_rot = rotary[rows:total, 0:rot].astype(F32)
    tiled_lat = jnp.concatenate([dkeys_lat] * heads, axis=0)
    tiled_rot = jnp.concatenate([dkeys_rot] * heads, axis=0)
    self_score = (
        jnp.sum(dq[:, 0:lat].astype(F32) * tiled_lat, axis=-1, keepdims=True)
        + jnp.sum(dq[:, lat:].astype(F32) * tiled_rot, axis=-1, keepdims=True)
    ) * scale
    row_of = lax.rem(lax.broadcasted_iota(jnp.int32, (drows, lat), 0), extra)
    dlat = jnp.zeros((drows, lat), F32)
    slots = r["dcache"].shape[2]
    for b in range(decodes):
        s = dot(dq, r["dcache"][b])
        live = lanes((drows, slots)) < r["lengths"][b]
        s = jnp.where(live, s * scale, NEG_FILL)
        m = jnp.maximum(jnp.max(s, axis=-1, keepdims=True), self_score)
        w = jnp.where(live, jnp.exp(s - m), 0.0)
        w_self = jnp.exp(self_score - m)
        norm = jnp.sum(w, axis=-1, keepdims=True) + w_self
        v = dot_t(w.astype(BF16), r["dcache"][b, 0:lat, :])
        v = (v + w_self.astype(BF16).astype(F32) * tiled_lat) / norm
        dlat = jnp.where(row_of == b, v, dlat)
    local["value_up"].wait()
    ho = r["ho"]
    for h in range(heads):
        ho[rows:total, h * vdim : (h + 1) * vdim] = dot_wide(
            dlat[h * extra : (h + 1) * extra], r["value_up"][h]
        ).astype(BF16)

    local["pcache"].wait()
    sendv, recvv, sends, recvs = r["sendv"], r["recvv"], r["sends"], r["recvs"]
    chunk = pair * rows
    qc = r["qc"]

    def value_copy(mine, peer):
        return pltpu.make_async_remote_copy(
            src_ref=sendv.at[peer], dst_ref=recvv.at[mine],
            send_sem=r["v_send"].at[peer], recv_sem=r["v_recv"].at[mine],
            device_id={"kv": peer}, device_id_type=MESH,
        )

    def stat_copy(mine, peer):
        return pltpu.make_async_remote_copy(
            src_ref=sends.at[peer], dst_ref=recvs.at[mine],
            send_sem=r["s_send"].at[peer], recv_sem=r["s_recv"].at[mine],
            device_id={"kv": peer}, device_id_type=MESH,
        )

    stat_lane = lanes((rows, 128))

    def stats(m, norm, t, start):
        out = jnp.zeros((rows, 128), F32)
        for h in range(heads):
            at = h * t + start
            out = jnp.where(stat_lane == h, m[at : at + rows], out)
            out = jnp.where(stat_lane == heads + h, norm[at : at + rows], out)
        return out

    def chunk_step(c, carry):
        base = lax.rem(lax.div(kv, pair) + c, n_kv // pair) * pair
        for i in range(pair):
            @pl.when(base + i != kv)
            def _():
                gather_copy(base + i, kv, 0).wait_recv()
        at = pl.ds(pl.multiple_of(base * rows, chunk), chunk)
        comp_rows = gath[pl.ds(base, pair), :, 0:qrank].reshape(chunk, qrank)
        make_queries(comp_rows, r["cos"][at, :], r["sin"][at, :], qc)
        s = dot(qc[...], r["pcache"][...]) * scale
        m = jnp.max(s, axis=-1, keepdims=True)
        w = jnp.exp(s - m)
        norm = jnp.sum(w, axis=-1, keepdims=True)
        v = dot_t(w.astype(BF16), r["pcache"][0:lat, :]).astype(BF16)
        for h in range(heads):
            pv = dot(v[h * chunk : (h + 1) * chunk], r["value_up"][h]).astype(BF16)
            for i in range(pair):
                sendv[base + i, :, h * vdim : (h + 1) * vdim] = pv[i * rows : (i + 1) * rows]
        for i in range(pair):
            sends[base + i] = stats(m, norm, chunk, i * rows)
        for i in range(pair):
            @pl.when(base + i != kv)
            def _():
                value_copy(kv, base + i).start()
                stat_copy(kv, base + i).start()
        return carry

    lax.fori_loop(0, n_kv // pair, chunk_step, 0)

    own_q = jnp.concatenate([qo[h * total : h * total + rows, :] for h in range(heads)], axis=0)
    every = gath[...].reshape(piece_total, gath.shape[2])
    key_lat = every[:, qrank : qrank + lat]
    s = dot_t(own_q[:, 0:lat], key_lat) + dot_t(own_q[:, lat:], every[:, qrank + lat : qrank + lat + rot])
    row = lax.rem(lax.broadcasted_iota(jnp.int32, s.shape, 0), rows) + kv * rows
    causal = lanes(s.shape) <= row
    s = jnp.where(causal, s * scale, NEG_FILL)
    m = jnp.max(s, axis=-1, keepdims=True)
    w = jnp.where(causal, jnp.exp(s - m), 0.0)
    norm = jnp.sum(w, axis=-1, keepdims=True)
    own_v = dot(w.astype(BF16), key_lat)
    own_stats = stats(m, norm, rows, 0)
    own_p = [dot_wide(own_v[h * rows : (h + 1) * rows], r["value_up"][h]) for h in range(heads)]

    recvv[kv] = sendv[kv]
    recvs[kv] = sends[kv]
    for d in range(1, n_kv):
        peer = lax.rem(kv + n_kv - d, n_kv)
        stat_copy(peer, kv).wait_recv()
        value_copy(peer, kv).wait_recv()
    joint = own_stats
    for j in range(n_kv):
        joint = jnp.maximum(joint, recvs[j])
    factor = jnp.exp(own_stats - joint)
    bottom = pltpu.roll(own_stats, 128 - heads, 1) * factor
    top = [own_p[h] * factor[:, h : h + 1] for h in range(heads)]
    for j in range(n_kv):
        st = recvs[j]
        factor = jnp.exp(st - joint)
        bottom = bottom + pltpu.roll(st, 128 - heads, 1) * factor
        for h in range(heads):
            top[h] = top[h] + recvv[j, :, h * vdim : (h + 1) * vdim].astype(F32) * factor[:, h : h + 1]
    for h in range(heads):
        ho[0:rows, h * vdim : (h + 1) * vdim] = (top[h] / bottom[:, h : h + 1]).astype(BF16)

    local["out_w"].wait()
    local["out_gain"].wait()
    mixs, mixr, sqs, sqr = r["mixs"], r["mixr"], r["sqs"], r["sqr"]
    cols = mixs.shape[2]

    def mix_copy(mine, peer):
        return pltpu.make_async_remote_copy(
            src_ref=mixs.at[peer], dst_ref=mixr.at[mine],
            send_sem=r["m_send"].at[peer], recv_sem=r["m_recv"].at[mine],
            device_id={"tp": peer}, device_id_type=MESH,
        )

    def square_copy(mine, peer):
        return pltpu.make_async_remote_copy(
            src_ref=sqs, dst_ref=sqr.at[mine],
            send_sem=r["q_send"].at[peer], recv_sem=r["q_recv"].at[mine],
            device_id={"tp": peer}, device_id_type=MESH,
        )

    head_out = ho[...]
    for d in range(1, n_tp):
        peer = lax.rem(tp + d, n_tp)
        at = pl.ds(pl.multiple_of(peer * cols, 128), cols)
        mixs[peer] = dot(head_out, r["out_w"][:, at]).astype(BF16)
        mix_copy(tp, peer).start()
    mix = dot(head_out, r["out_w"][:, pl.ds(pl.multiple_of(tp * cols, 128), cols)])
    for d in range(1, n_tp):
        peer = lax.rem(tp + n_tp - d, n_tp)
        mix_copy(peer, tp).wait_recv()
        mix = mix + mixr[peer].astype(F32)
    squares = jnp.sum(mix * mix, axis=-1, keepdims=True)
    sqs[...] = jnp.broadcast_to(squares, sqs.shape)
    for d in range(1, n_tp):
        square_copy(tp, lax.rem(tp + d, n_tp)).start()
    for d in range(1, n_tp):
        peer = lax.rem(tp + n_tp - d, n_tp)
        square_copy(peer, tp).wait_recv()
        squares = squares + sqr[peer][:, 0:1]
    result = mix * lax.rsqrt(squares / (cols * n_tp) + EPSILON) * r["out_gain"][...]
    r["piece_out"][...] = result[0:rows]
    r["decode_out"][...] = result[rows : rows + decodes]

    for d in range(1, n_kv):
        peer = lax.rem(kv + d, n_kv)
        gather_copy(kv, peer, d).wait_send()
        value_copy(kv, peer).wait_send()
        stat_copy(kv, peer).wait_send()
    for d in range(1, n_tp):
        peer = lax.rem(tp + d, n_tp)
        mix_copy(tp, peer).wait_send()
        square_copy(tp, peer).wait_send()


def finish(*refs):
    count = len(refs) // 2
    for i in range(count):
        refs[count + i][...] = refs[i][...]


def shards(
    n_kv, n_tp,
    piece_tokens, decode_tokens, decode_lengths, prompt_cache, decode_cache, input_gain,
    query_down, query_gain, query_nope_weight, query_rope_weight, latent_weight, latent_gain,
    rotary_weight, key_up, value_up, out_weight, out_gain,
):
    rows, model = piece_tokens.shape
    decodes = decode_tokens.shape[0]
    extra = -(-decodes // 16) * 16
    total = rows + extra
    heads = key_up.shape[0]
    lat = latent_gain.shape[0]
    qrank = query_gain.shape[0]
    rot = rotary_weight.shape[1]
    pair = 2 if n_kv % 2 == 0 else 1
    wide = -(-rot // 128) * 128
    cols = out_gain.shape[0]

    args = {
        "lengths": decode_lengths,
        "piece": piece_tokens, "decode": decode_tokens, "input_gain": input_gain[None],
        "down": query_down, "query_gain": query_gain[None], "latent": latent_weight,
        "latent_gain": latent_gain[None], "rotary": rotary_weight.T,
        "nope": query_nope_weight, "rope": query_rope_weight, "key_up": key_up,
        "dcache": decode_cache.transpose(0, 2, 1), "pcache": prompt_cache.T, "value_up": value_up,
        "out_w": out_weight, "out_gain": out_gain[None],
    }
    outs = {
        "piece_out": ((rows, cols), F32), "decode_out": ((decodes, cols), F32),
        "piece_keys": ((rows, lat + rot), BF16), "decode_keys": ((decodes, lat + rot), BF16),
    }
    width = lat + rot
    vdim = value_up.shape[2]
    scratch = {k: pltpu.VMEM(v.shape, v.dtype) for k, v in args.items() if k != "lengths"}
    scratch |= {
        "tok": pltpu.VMEM((total, model), F32),
        "cos": pltpu.VMEM((rows * n_kv + extra, 128), F32),
        "sin": pltpu.VMEM((rows * n_kv + extra, 128), F32),
        "rk": pltpu.VMEM((total, 128), F32),
        "tab": pltpu.VMEM((2, total, 128), F32),
        "gath": pltpu.VMEM((n_kv, rows, qrank + lat + wide), BF16),
        "qo": pltpu.VMEM((heads * total, width), BF16),
        "qc": pltpu.VMEM((heads * pair * rows, width), BF16),
        "ho": pltpu.VMEM((total, heads * vdim), BF16),
        "sendv": pltpu.VMEM((n_kv, rows, heads * vdim), BF16),
        "recvv": pltpu.VMEM((n_kv, rows, heads * vdim), BF16),
        "sends": pltpu.VMEM((n_kv, rows, 128), F32),
        "recvs": pltpu.VMEM((n_kv, rows, 128), F32),
        "mixs": pltpu.VMEM((n_tp, total, cols), BF16),
        "mixr": pltpu.VMEM((n_tp, total, cols), BF16),
        "sqs": pltpu.VMEM((total, 128), F32),
        "sqr": pltpu.VMEM((n_tp, total, 128), F32),
        "load_sem": pltpu.SemaphoreType.DMA((len(args) - 1,)),
    }
    for k in ("g", "v", "s"):
        scratch[k + "_send"] = pltpu.SemaphoreType.DMA((n_kv,))
        scratch[k + "_recv"] = pltpu.SemaphoreType.DMA((n_kv,))
    for k in ("m", "q"):
        scratch[k + "_send"] = pltpu.SemaphoreType.DMA((n_tp,))
        scratch[k + "_recv"] = pltpu.SemaphoreType.DMA((n_tp,))
    names = [k if k == "lengths" else k + "_hbm" for k in args] + list(outs) + list(scratch)
    results = pl.pallas_call(
        functools.partial(kernel, n_kv, n_tp, pair, names),
        out_shape=[jax.ShapeDtypeStruct(*v) for v in outs.values()],
        in_specs=[
            pl.BlockSpec(memory_space=pltpu.SMEM if k == "lengths" else pl.ANY) for k in args
        ],
        out_specs=[pl.BlockSpec(memory_space=pltpu.VMEM) for _ in outs],
        scratch_shapes=list(scratch.values()),
        compiler_params=pltpu.CompilerParams(
            collective_id=0, has_side_effects=True, vmem_limit_bytes=60000 * 1024
        ),
    )(*args.values())
    return pl.pallas_call(
        finish,
        out_shape=[jax.ShapeDtypeStruct(*v) for v in outs.values()],
        in_specs=[pl.BlockSpec(memory_space=pltpu.VMEM) for _ in outs],
        out_specs=[pl.BlockSpec(memory_space=pltpu.VMEM) for _ in outs],
    )(*results)


def solution(mesh):
    in_specs = (
        P("kv", None), P("kv", None), P("kv"), P("kv", None), P("kv", None, None), P(), P(), P(),
        P(None, "tp"), P(None, "tp"), P(), P(), P(), P("tp", None, None), P("tp", None, None),
        P("tp", None), P("tp"),
    )
    out_specs = (P("kv", "tp"), P("kv", "tp"), P("kv", None), P("kv", None))
    body = functools.partial(shards, mesh.shape["kv"], mesh.shape["tp"])
    return jax.shard_map(
        body, mesh=mesh, in_specs=in_specs, out_specs=out_specs, check_vma=False
    )
```

```python
import functools

import jax
import jax.numpy as jnp
from jax import lax
from jax.experimental import pallas as pl
from jax.experimental.pallas import tpu as pltpu
from jax.sharding import PartitionSpec as P

EPSILON = 1e-06
NEG_FILL = -1e30
ROPE_BASE = 10000.0
MESH = pl.DeviceIdType.MESH
F32 = jnp.float32
BF16 = jnp.bfloat16


def dot(a, b):
    return jnp.dot(a, b, preferred_element_type=F32)


def dot_t(a, b):
    return lax.dot_general(a, b, (((1,), (1,)), ((), ())), preferred_element_type=F32)


def dot_wide(a, b):
    high = a.astype(BF16)
    low = (a - high.astype(F32)).astype(BF16)
    return dot(high, b) + dot(low, b)


def rms(x, gain):
    return x * lax.rsqrt(jnp.mean(x * x, axis=-1, keepdims=True) + EPSILON) * gain


def lanes(shape):
    return lax.broadcasted_iota(jnp.int32, shape, len(shape) - 1)


def swap_halves(x, rotary):
    width = x.shape[-1]
    half = rotary // 2
    first = lax.rem(lanes(x.shape), rotary) < half
    return jnp.where(first, pltpu.roll(x, width - half, 1), pltpu.roll(x, half, 1))


def kernel(n_kv, n_tp, pair, names, *refs):
    r = dict(zip(names, refs))
    kv = lax.axis_index("kv")
    tp = lax.axis_index("tp")
    loads = (
        "piece", "decode", "input_gain", "down", "query_gain", "latent", "latent_gain",
        "rotary", "nope", "rope", "key_up", "dcache", "pcache", "value_up",
        "out_w", "out_gain",
    )
    local = {
        name: pltpu.make_async_copy(r[name + "_hbm"], r[name], r["load_sem"].at[i])
        for i, name in enumerate(loads)
    }
    late = loads.index("dcache")
    for name in loads[:late]:
        local[name].start()
    barrier = pltpu.get_barrier_semaphore()
    for d in range(1, n_kv):
        pl.semaphore_signal(
            barrier, inc=1, device_id={"kv": lax.rem(kv + d, n_kv)}, device_id_type=MESH
        )
    for d in range(1, n_tp):
        pl.semaphore_signal(
            barrier, inc=1, device_id={"tp": lax.rem(tp + d, n_tp)}, device_id_type=MESH
        )

    rows = r["piece"].shape[0]
    decodes = r["decode"].shape[0]
    extra = r["tok"].shape[0] - rows
    total = rows + extra
    lat = r["latent"].shape[1]
    qrank = r["down"].shape[1]
    rot = r["rotary"].shape[0]
    heads, nope_w = r["key_up"].shape[0], r["key_up"].shape[1]
    vdim = r["value_up"].shape[2]
    scale = (nope_w + rot) ** (-0.5)
    gcomp, gkeys = r["gcomp"], r["gkeys"]
    wide = gkeys.shape[2] - lat
    share = 2 if n_tp % 2 == 0 and rows % 32 == 0 else 1
    part_rows = rows // share
    mine = pl.ds(pl.multiple_of(lax.rem(tp, share) * part_rows, part_rows), part_rows)
    other = pl.ds(
        pl.multiple_of((share - 1 - lax.rem(tp, share)) * part_rows, part_rows), part_rows
    )
    partner = tp + 1 - 2 * lax.rem(tp, 2)

    piece_total = n_kv * rows
    shape = r["cos"].shape
    row_at = lax.broadcasted_iota(jnp.int32, shape, 0)
    position = row_at + r["pcache"].shape[1] * n_kv
    for b in range(decodes):
        position = jnp.where(row_at == piece_total + b, r["lengths"][b], position)
    lane = lanes((1, shape[1]))
    inverse = ROPE_BASE ** (-lax.rem(lane, rot // 2).astype(F32) / (rot // 2))
    angle = position.astype(F32) * inverse
    r["cos"][...] = jnp.cos(angle)
    sine = jnp.sin(angle)
    r["sin"][...] = jnp.where(lax.rem(lanes(shape), rot) < rot // 2, -sine, sine)

    tok = r["tok"]
    local["piece"].wait()
    local["decode"].wait()
    local["input_gain"].wait()
    tok[0:rows, :] = r["piece"][...].astype(F32)
    tok[rows:total, :] = jnp.zeros((extra, tok.shape[1]), F32)
    tok[rows : rows + decodes, :] = r["decode"][...].astype(F32)
    normed = rms(tok[...], r["input_gain"][...]).astype(BF16)
    local["down"].wait()
    local["query_gain"].wait()
    comp = rms(dot(normed, r["down"][...]), r["query_gain"][...]).astype(BF16)
    local["latent"].wait()
    local["latent_gain"].wait()
    for name in loads[late:]:
        local[name].start()
    latent = rms(dot(normed, r["latent"][...]), r["latent_gain"][...]).astype(BF16)
    local["rotary"].wait()
    rk = r["rk"]
    rk[...] = jnp.zeros(rk.shape, F32)
    rk[:, 0:rot] = dot_t(normed, r["rotary"][...])
    own_rows = pl.ds(pl.multiple_of(kv * rows, rows), rows)
    tab = r["tab"]
    tab[0, 0:rows, :] = r["cos"][own_rows, :]
    tab[0, rows:total, :] = r["cos"][piece_total : piece_total + extra, :]
    tab[1, 0:rows, :] = r["sin"][own_rows, :]
    tab[1, rows:total, :] = r["sin"][piece_total : piece_total + extra, :]
    raw = rk[...]
    rotary = (raw * tab[0, :, 0 : rk.shape[1]] + swap_halves(raw, rot) * tab[1, :, 0 : rk.shape[1]]).astype(BF16)
    gcomp[kv] = comp[0:rows]
    gkeys[kv, :, 0:lat] = latent[0:rows]
    gkeys[kv, :, lat:] = rotary[0:rows, 0:wide]

    def gather_copy(buf, tag, slot, peer, d):
        return pltpu.make_async_remote_copy(
            src_ref=buf.at[slot, mine], dst_ref=buf.at[slot, mine],
            send_sem=r[tag + "_send"].at[d], recv_sem=r[tag + "_recv"].at[slot],
            device_id={"kv": peer}, device_id_type=MESH,
        )

    def forward_copy(buf, tag, slot, part):
        return pltpu.make_async_remote_copy(
            src_ref=buf.at[slot, part], dst_ref=buf.at[slot, part],
            send_sem=r[tag + "_send"].at[slot], recv_sem=r[tag + "_recv"].at[slot],
            device_id={"tp": partner}, device_id_type=MESH,
        )

    def forward(buf, tag, slot):
        gather_copy(buf, tag, slot, kv, 0).wait_recv()
        if share == 2:
            forward_copy(buf, tag + "f", slot, mine).start()

    def forwarded(buf, tag, slot):
        if share == 2:
            forward_copy(buf, tag + "f", slot, other).wait_recv()

    chunks = n_kv // pair

    def base_of(c):
        return lax.rem(lax.div(kv, pair) + c, chunks) * pair

    def forward_chunk(c):
        base = base_of(c)
        for i in range(pair):
            @pl.when(base + i != kv)
            def _():
                forward(gcomp, "g", base + i)

    pl.semaphore_wait(barrier, n_kv - 1 + n_tp - 1)
    for d in range(1, n_kv):
        gather_copy(gcomp, "g", kv, lax.rem(kv + d, n_kv), d).start()
    for d in range(1, n_kv):
        gather_copy(gkeys, "k", kv, lax.rem(kv + d, n_kv), d).start()

    r["piece_keys"][:, 0:lat] = latent[0:rows]
    r["piece_keys"][:, lat:] = rotary[0:rows, 0:rot]
    r["decode_keys"][:, 0:lat] = latent[rows : rows + decodes]
    r["decode_keys"][:, lat:] = rotary[rows : rows + decodes, 0:rot]

    local["nope"].wait()
    local["rope"].wait()
    local["key_up"].wait()

    def make_queries(comp_rows, cosine, sine, q_ref):
        t = comp_rows.shape[0]
        qn = dot(comp_rows, r["nope"][...]).astype(BF16)
        qr = dot(comp_rows, r["rope"][...])
        width = qr.shape[1]
        reps = width // cosine.shape[1]
        cosine = jnp.concatenate([cosine] * reps, axis=1)
        sine = jnp.concatenate([sine] * reps, axis=1)
        qr = qr * cosine + swap_halves(qr, rot) * sine
        for h in range(heads):
            q_ref[h * t : (h + 1) * t, 0:lat] = dot(
                qn[:, h * nope_w : (h + 1) * nope_w], r["key_up"][h]
            ).astype(BF16)
            shift = (width - h * rot) % width
            part = pltpu.roll(qr, shift, 1) if shift else qr
            q_ref[h * t : (h + 1) * t, lat:] = part[:, 0:rot].astype(BF16)

    qo = r["qo"]
    make_queries(comp, tab[0], tab[1], qo)
    dq = jnp.concatenate([qo[h * total + rows : (h + 1) * total, :] for h in range(heads)], axis=0)
    drows = heads * extra

    local["dcache"].wait()
    dkeys_lat = latent[rows:total].astype(F32)
    dkeys_rot = rotary[rows:total, 0:rot].astype(F32)
    tiled_lat = jnp.concatenate([dkeys_lat] * heads, axis=0)
    tiled_rot = jnp.concatenate([dkeys_rot] * heads, axis=0)
    self_score = (
        jnp.sum(dq[:, 0:lat].astype(F32) * tiled_lat, axis=-1, keepdims=True)
        + jnp.sum(dq[:, lat:].astype(F32) * tiled_rot, axis=-1, keepdims=True)
    ) * scale
    row_of = lax.rem(lax.broadcasted_iota(jnp.int32, (drows, lat), 0), extra)
    dlat = jnp.zeros((drows, lat), F32)
    slots = r["dcache"].shape[2]
    for b in range(decodes):
        s = dot(dq, r["dcache"][b])
        live = lanes((drows, slots)) < r["lengths"][b]
        s = jnp.where(live, s * scale, NEG_FILL)
        m = jnp.maximum(jnp.max(s, axis=-1, keepdims=True), self_score)
        w = jnp.where(live, jnp.exp(s - m), 0.0)
        w_self = jnp.exp(self_score - m)
        norm = jnp.sum(w, axis=-1, keepdims=True) + w_self
        v = dot_t(w.astype(BF16), r["dcache"][b, 0:lat, :])
        v = (v + w_self.astype(BF16).astype(F32) * tiled_lat) / norm
        dlat = jnp.where(row_of == b, v, dlat)
        if b == 0:
            forward_chunk(0)
    local["value_up"].wait()
    ho = r["ho"]
    for h in range(heads):
        ho[rows:total, h * vdim : (h + 1) * vdim] = dot_wide(
            dlat[h * extra : (h + 1) * extra], r["value_up"][h]
        ).astype(BF16)

    local["pcache"].wait()
    sendv, recvv = r["sendv"], r["recvv"]
    chunk = pair * rows
    qc = r["qc"]

    def value_copy(mine, peer):
        return pltpu.make_async_remote_copy(
            src_ref=sendv.at[peer], dst_ref=recvv.at[mine],
            send_sem=r["v_send"].at[peer], recv_sem=r["v_recv"].at[mine],
            device_id={"kv": peer}, device_id_type=MESH,
        )

    stat_lane = lanes((rows, 128))

    def stats(m, norm, t, start):
        out = jnp.zeros((rows, 128), F32)
        for h in range(heads):
            at = h * t + start
            out = jnp.where(stat_lane == h, m[at : at + rows], out)
            out = jnp.where(stat_lane == heads + h, norm[at : at + rows], out)
        return out

    def chunk_step(c, carry):
        base = base_of(c)

        @pl.when(c + 1 < chunks)
        def _():
            forward_chunk(c + 1)

        @pl.when(c + 1 == chunks)
        def _():
            for d in range(1, n_kv):
                forward(gkeys, "k", lax.rem(kv + d, n_kv))

        for i in range(pair):
            @pl.when(base + i != kv)
            def _():
                forwarded(gcomp, "g", base + i)
        at = pl.ds(pl.multiple_of(base * rows, chunk), chunk)
        comp_rows = gcomp[pl.ds(base, pair)].reshape(chunk, qrank)
        make_queries(comp_rows, r["cos"][at, :], r["sin"][at, :], qc)
        s = dot(qc[...], r["pcache"][...]) * scale
        m = jnp.max(s, axis=-1, keepdims=True)
        w = jnp.exp(s - m)
        norm = jnp.sum(w, axis=-1, keepdims=True)
        v = dot_t(w.astype(BF16), r["pcache"][0:lat, :]).astype(BF16)
        for h in range(heads):
            pv = dot(v[h * chunk : (h + 1) * chunk], r["value_up"][h]).astype(BF16)
            for i in range(pair):
                sendv[base + i, :, h * vdim : (h + 1) * vdim] = pv[i * rows : (i + 1) * rows]
        for i in range(pair):
            st = stats(m, norm, chunk, i * rows)
            high = st.astype(BF16).astype(F32)
            mid = (st - high).astype(BF16).astype(F32)
            low = (st - high) - mid
            packed = high + pltpu.roll(mid, 2 * heads, 1) + pltpu.roll(low, 4 * heads, 1)
            sendv[base + i, :, heads * vdim :] = packed.astype(BF16)
        for i in range(pair):
            @pl.when(base + i != kv)
            def _():
                value_copy(kv, base + i).start()
        return carry

    lax.fori_loop(0, n_kv // pair, chunk_step, 0)

    own_q = jnp.concatenate([qo[h * total : h * total + rows, :] for h in range(heads)], axis=0)
    for d in range(1, n_kv):
        forwarded(gkeys, "k", lax.rem(kv + d, n_kv))
    every = gkeys[...].reshape(piece_total, gkeys.shape[2])
    key_lat = every[:, 0:lat]
    s = dot_t(own_q[:, 0:lat], key_lat) + dot_t(own_q[:, lat:], every[:, lat : lat + rot])
    row = lax.rem(lax.broadcasted_iota(jnp.int32, s.shape, 0), rows) + kv * rows
    causal = lanes(s.shape) <= row
    s = jnp.where(causal, s * scale, NEG_FILL)
    m = jnp.max(s, axis=-1, keepdims=True)
    w = jnp.where(causal, jnp.exp(s - m), 0.0)
    norm = jnp.sum(w, axis=-1, keepdims=True)
    own_v = dot(w.astype(BF16), key_lat)
    own_stats = stats(m, norm, rows, 0)
    own_p = [dot_wide(own_v[h * rows : (h + 1) * rows], r["value_up"][h]) for h in range(heads)]

    recvv[kv] = sendv[kv]
    for d in range(1, n_kv):
        peer = lax.rem(kv + n_kv - d, n_kv)
        value_copy(peer, kv).wait_recv()
    joint = own_stats
    received = []
    for j in range(n_kv):
        st = recvv[j, :, heads * vdim :].astype(F32)
        st = st + pltpu.roll(st, 128 - 2 * heads, 1) + pltpu.roll(st, 128 - 4 * heads, 1)
        received.append(jnp.where(stat_lane < 2 * heads, st, 0.0))
        joint = jnp.maximum(joint, received[j])
    factor = jnp.exp(own_stats - joint)
    bottom = pltpu.roll(own_stats, 128 - heads, 1) * factor
    top = [own_p[h] * factor[:, h : h + 1] for h in range(heads)]
    for j in range(n_kv):
        st = received[j]
        factor = jnp.exp(st - joint)
        bottom = bottom + pltpu.roll(st, 128 - heads, 1) * factor
        for h in range(heads):
            top[h] = top[h] + recvv[j, :, h * vdim : (h + 1) * vdim].astype(F32) * factor[:, h : h + 1]
    for h in range(heads):
        ho[0:rows, h * vdim : (h + 1) * vdim] = (top[h] / bottom[:, h : h + 1]).astype(BF16)

    local["out_w"].wait()
    local["out_gain"].wait()
    mixs, mixr, sqs, sqr = r["mixs"], r["mixr"], r["sqs"], r["sqr"]
    cols = mixs.shape[2]

    def mix_copy(mine, peer):
        return pltpu.make_async_remote_copy(
            src_ref=mixs.at[peer], dst_ref=mixr.at[mine],
            send_sem=r["m_send"].at[peer], recv_sem=r["m_recv"].at[mine],
            device_id={"tp": peer}, device_id_type=MESH,
        )

    def square_copy(mine, peer):
        return pltpu.make_async_remote_copy(
            src_ref=sqs, dst_ref=sqr.at[mine],
            send_sem=r["q_send"].at[peer], recv_sem=r["q_recv"].at[mine],
            device_id={"tp": peer}, device_id_type=MESH,
        )

    head_out = ho[...]
    for d in range(1, n_tp):
        peer = lax.rem(tp + d, n_tp)
        at = pl.ds(pl.multiple_of(peer * cols, 128), cols)
        mixs[peer] = dot(head_out, r["out_w"][:, at]).astype(BF16)
        mix_copy(tp, peer).start()
    mix = dot(head_out, r["out_w"][:, pl.ds(pl.multiple_of(tp * cols, 128), cols)])
    for d in range(1, n_tp):
        peer = lax.rem(tp + n_tp - d, n_tp)
        mix_copy(peer, tp).wait_recv()
        mix = mix + mixr[peer].astype(F32)
    squares = jnp.sum(mix * mix, axis=-1, keepdims=True)
    diagonal = lax.broadcasted_iota(jnp.int32, (total, 128), 0) == lanes((total, 128))
    sqs[...] = jnp.broadcast_to(
        jnp.sum(jnp.where(diagonal, squares, 0.0), axis=0, keepdims=True), sqs.shape
    )
    for d in range(1, n_tp):
        square_copy(tp, lax.rem(tp + d, n_tp)).start()
    square_row = sqs[0:1, :]
    for d in range(1, n_tp):
        peer = lax.rem(tp + n_tp - d, n_tp)
        square_copy(peer, tp).wait_recv()
        square_row = square_row + sqr[peer, 0:1, :]
    squares = jnp.sum(jnp.where(diagonal, square_row, 0.0), axis=1, keepdims=True)
    result = mix * lax.rsqrt(squares / (cols * n_tp) + EPSILON) * r["out_gain"][...]
    r["piece_out"][...] = result[0:rows]
    r["decode_out"][...] = result[rows : rows + decodes]

    for d in range(1, n_kv):
        peer = lax.rem(kv + d, n_kv)
        gather_copy(gcomp, "g", kv, peer, d).wait_send()
        gather_copy(gkeys, "k", kv, peer, d).wait_send()
        if share == 2:
            forward_copy(gcomp, "gf", peer, mine).wait_send()
            forward_copy(gkeys, "kf", peer, mine).wait_send()
        value_copy(kv, peer).wait_send()
    for d in range(1, n_tp):
        peer = lax.rem(tp + d, n_tp)
        mix_copy(tp, peer).wait_send()
        square_copy(tp, peer).wait_send()


def finish(*refs):
    count = len(refs) // 2
    for i in range(count):
        refs[count + i][...] = refs[i][...]


def shards(
    n_kv, n_tp,
    piece_tokens, decode_tokens, decode_lengths, prompt_cache, decode_cache, input_gain,
    query_down, query_gain, query_nope_weight, query_rope_weight, latent_weight, latent_gain,
    rotary_weight, key_up, value_up, out_weight, out_gain,
):
    rows, model = piece_tokens.shape
    decodes = decode_tokens.shape[0]
    extra = -(-decodes // 16) * 16
    total = rows + extra
    heads = key_up.shape[0]
    lat = latent_gain.shape[0]
    qrank = query_gain.shape[0]
    rot = rotary_weight.shape[1]
    pair = 2 if n_kv % 2 == 0 else 1
    wide = -(-rot // 128) * 128
    cols = out_gain.shape[0]

    args = {
        "lengths": decode_lengths,
        "piece": piece_tokens, "decode": decode_tokens, "input_gain": input_gain[None],
        "down": query_down, "query_gain": query_gain[None], "latent": latent_weight,
        "latent_gain": latent_gain[None], "rotary": rotary_weight.T,
        "nope": query_nope_weight, "rope": query_rope_weight, "key_up": key_up,
        "dcache": decode_cache.transpose(0, 2, 1), "pcache": prompt_cache.T, "value_up": value_up,
        "out_w": out_weight, "out_gain": out_gain[None],
    }
    outs = {
        "piece_out": ((rows, cols), F32), "decode_out": ((decodes, cols), F32),
        "piece_keys": ((rows, lat + rot), BF16), "decode_keys": ((decodes, lat + rot), BF16),
    }
    width = lat + rot
    vdim = value_up.shape[2]
    scratch = {k: pltpu.VMEM(v.shape, v.dtype) for k, v in args.items() if k != "lengths"}
    scratch |= {
        "tok": pltpu.VMEM((total, model), F32),
        "cos": pltpu.VMEM((rows * n_kv + extra, 128), F32),
        "sin": pltpu.VMEM((rows * n_kv + extra, 128), F32),
        "rk": pltpu.VMEM((total, 128), F32),
        "tab": pltpu.VMEM((2, total, 128), F32),
        "gcomp": pltpu.VMEM((n_kv, rows, qrank), BF16),
        "gkeys": pltpu.VMEM((n_kv, rows, lat + wide), BF16),
        "qo": pltpu.VMEM((heads * total, width), BF16),
        "qc": pltpu.VMEM((heads * pair * rows, width), BF16),
        "ho": pltpu.VMEM((total, heads * vdim), BF16),
        "sendv": pltpu.VMEM((n_kv, rows, heads * vdim + 128), BF16),
        "recvv": pltpu.VMEM((n_kv, rows, heads * vdim + 128), BF16),
        "mixs": pltpu.VMEM((n_tp, total, cols), BF16),
        "mixr": pltpu.VMEM((n_tp, total, cols), BF16),
        "sqs": pltpu.VMEM((8, 128), F32),
        "sqr": pltpu.VMEM((n_tp, 8, 128), F32),
        "load_sem": pltpu.SemaphoreType.DMA((len(args) - 1,)),
    }
    for k in ("g", "k", "gf", "kf", "v"):
        scratch[k + "_send"] = pltpu.SemaphoreType.DMA((n_kv,))
        scratch[k + "_recv"] = pltpu.SemaphoreType.DMA((n_kv,))
    for k in ("m", "q"):
        scratch[k + "_send"] = pltpu.SemaphoreType.DMA((n_tp,))
        scratch[k + "_recv"] = pltpu.SemaphoreType.DMA((n_tp,))
    names = [k if k == "lengths" else k + "_hbm" for k in args] + list(outs) + list(scratch)
    results = pl.pallas_call(
        functools.partial(kernel, n_kv, n_tp, pair, names),
        out_shape=[jax.ShapeDtypeStruct(*v) for v in outs.values()],
        in_specs=[
            pl.BlockSpec(memory_space=pltpu.SMEM if k == "lengths" else pl.ANY) for k in args
        ],
        out_specs=[pl.BlockSpec(memory_space=pltpu.VMEM) for _ in outs],
        scratch_shapes=list(scratch.values()),
        compiler_params=pltpu.CompilerParams(
            collective_id=0, has_side_effects=True, vmem_limit_bytes=60000 * 1024
        ),
    )(*args.values())
    return pl.pallas_call(
        finish,
        out_shape=[jax.ShapeDtypeStruct(*v) for v in outs.values()],
        in_specs=[pl.BlockSpec(memory_space=pltpu.VMEM) for _ in outs],
        out_specs=[pl.BlockSpec(memory_space=pltpu.VMEM) for _ in outs],
    )(*results)


def solution(mesh):
    in_specs = (
        P("kv", None), P("kv", None), P("kv"), P("kv", None), P("kv", None, None), P(), P(), P(),
        P(None, "tp"), P(None, "tp"), P(), P(), P(), P("tp", None, None), P("tp", None, None),
        P("tp", None), P("tp"),
    )
    out_specs = (P("kv", "tp"), P("kv", "tp"), P("kv", None), P("kv", None))
    body = functools.partial(shards, mesh.shape["kv"], mesh.shape["tp"])
    return jax.shard_map(
        body, mesh=mesh, in_specs=in_specs, out_specs=out_specs, check_vma=False
    )
```

```python
import functools

import jax
import jax.numpy as jnp
from jax import lax
from jax.experimental import pallas as pl
from jax.experimental.pallas import tpu as pltpu
from jax.sharding import PartitionSpec as P

EPSILON = 1e-06
NEG_FILL = -1e30
ROPE_BASE = 10000.0
MESH = pl.DeviceIdType.MESH
F32 = jnp.float32
BF16 = jnp.bfloat16


def dot(a, b):
    return jnp.dot(a, b, preferred_element_type=F32)


def dot_t(a, b):
    return lax.dot_general(a, b, (((1,), (1,)), ((), ())), preferred_element_type=F32)


def dot_wide(a, b):
    high = a.astype(BF16)
    low = (a - high.astype(F32)).astype(BF16)
    return dot(high, b) + dot(low, b)


def rms(x, gain):
    return x * lax.rsqrt(jnp.mean(x * x, axis=-1, keepdims=True) + EPSILON) * gain


def lanes(shape):
    return lax.broadcasted_iota(jnp.int32, shape, len(shape) - 1)


def swap_halves(x, rotary):
    width = x.shape[-1]
    half = rotary // 2
    first = lax.rem(lanes(x.shape), rotary) < half
    return jnp.where(first, pltpu.roll(x, width - half, 1), pltpu.roll(x, half, 1))


def kernel(n_kv, n_tp, pair, names, *refs):
    r = dict(zip(names, refs))
    kv = lax.axis_index("kv")
    tp = lax.axis_index("tp")
    loads = (
        "piece", "decode", "input_gain", "down", "query_gain", "latent", "latent_gain",
        "rotary", "nope", "rope", "key_up", "dcache", "pcache", "value_up",
        "out_w", "out_gain",
    )
    local = {
        name: pltpu.make_async_copy(r[name + "_hbm"], r[name], r["load_sem"].at[i])
        for i, name in enumerate(loads)
    }
    late = loads.index("dcache")
    for name in loads[:late]:
        local[name].start()
    barrier = pltpu.get_barrier_semaphore()
    for d in range(1, n_kv):
        pl.semaphore_signal(
            barrier, inc=1, device_id={"kv": lax.rem(kv + d, n_kv)}, device_id_type=MESH
        )
    for d in range(1, n_tp):
        pl.semaphore_signal(
            barrier, inc=1, device_id={"tp": lax.rem(tp + d, n_tp)}, device_id_type=MESH
        )

    rows = r["piece"].shape[0]
    decodes = r["decode"].shape[0]
    extra = r["tok"].shape[0] - rows
    total = rows + extra
    lat = r["latent"].shape[1]
    qrank = r["down"].shape[1]
    rot = r["rotary"].shape[0]
    heads, nope_w = r["key_up"].shape[0], r["key_up"].shape[1]
    vdim = r["value_up"].shape[2]
    scale = (nope_w + rot) ** (-0.5)
    gcomp, gkeys = r["gcomp"], r["gkeys"]
    wide = gkeys.shape[2] - lat
    share = 2 if n_tp % 2 == 0 and rows % 32 == 0 else 1
    part_rows = rows // share
    mine = pl.ds(pl.multiple_of(lax.rem(tp, share) * part_rows, part_rows), part_rows)
    other = pl.ds(
        pl.multiple_of((share - 1 - lax.rem(tp, share)) * part_rows, part_rows), part_rows
    )
    partner = tp + 1 - 2 * lax.rem(tp, 2)

    piece_total = n_kv * rows
    shape = r["cos"].shape
    row_at = lax.broadcasted_iota(jnp.int32, shape, 0)
    position = row_at + r["pcache"].shape[1] * n_kv
    for b in range(decodes):
        position = jnp.where(row_at == piece_total + b, r["lengths"][b], position)
    lane = lanes((1, shape[1]))
    inverse = ROPE_BASE ** (-lax.rem(lane, rot // 2).astype(F32) / (rot // 2))
    angle = position.astype(F32) * inverse
    r["cos"][...] = jnp.cos(angle)
    sine = jnp.sin(angle)
    r["sin"][...] = jnp.where(lax.rem(lanes(shape), rot) < rot // 2, -sine, sine)

    tok = r["tok"]
    local["piece"].wait()
    local["decode"].wait()
    local["input_gain"].wait()
    tok[0:rows, :] = r["piece"][...].astype(F32)
    tok[rows:total, :] = jnp.zeros((extra, tok.shape[1]), F32)
    tok[rows : rows + decodes, :] = r["decode"][...].astype(F32)
    normed = rms(tok[...], r["input_gain"][...]).astype(BF16)
    local["down"].wait()
    local["query_gain"].wait()
    comp = rms(dot(normed, r["down"][...]), r["query_gain"][...]).astype(BF16)
    local["latent"].wait()
    local["latent_gain"].wait()
    for name in loads[late:]:
        local[name].start()
    latent = rms(dot(normed, r["latent"][...]), r["latent_gain"][...]).astype(BF16)
    local["rotary"].wait()
    rk = r["rk"]
    rk[...] = jnp.zeros(rk.shape, F32)
    rk[:, 0:rot] = dot_t(normed, r["rotary"][...])
    own_rows = pl.ds(pl.multiple_of(kv * rows, rows), rows)
    tab = r["tab"]
    tab[0, 0:rows, :] = r["cos"][own_rows, :]
    tab[0, rows:total, :] = r["cos"][piece_total : piece_total + extra, :]
    tab[1, 0:rows, :] = r["sin"][own_rows, :]
    tab[1, rows:total, :] = r["sin"][piece_total : piece_total + extra, :]
    raw = rk[...]
    rotary = (raw * tab[0, :, 0 : rk.shape[1]] + swap_halves(raw, rot) * tab[1, :, 0 : rk.shape[1]]).astype(BF16)
    gcomp[kv] = comp[0:rows]
    gkeys[kv, :, 0:lat] = latent[0:rows]
    gkeys[kv, :, lat:] = rotary[0:rows, 0:wide]

    def gather_copy(buf, tag, slot, peer, d):
        return pltpu.make_async_remote_copy(
            src_ref=buf.at[slot, mine], dst_ref=buf.at[slot, mine],
            send_sem=r[tag + "_send"].at[d], recv_sem=r[tag + "_recv"].at[slot],
            device_id={"kv": peer}, device_id_type=MESH,
        )

    def forward_copy(buf, tag, slot, part):
        return pltpu.make_async_remote_copy(
            src_ref=buf.at[slot, part], dst_ref=buf.at[slot, part],
            send_sem=r[tag + "_send"].at[slot], recv_sem=r[tag + "_recv"].at[slot],
            device_id={"tp": partner}, device_id_type=MESH,
        )

    def forward(buf, tag, slot):
        gather_copy(buf, tag, slot, kv, 0).wait_recv()
        if share == 2:
            forward_copy(buf, tag + "f", slot, mine).start()

    def forwarded(buf, tag, slot):
        if share == 2:
            forward_copy(buf, tag + "f", slot, other).wait_recv()

    chunks = n_kv // pair

    def base_of(c):
        sign = 2 * lax.rem(c, 2) - 1
        shift = lax.rem(chunks // 2 + lax.div(c + 1, 2) * sign + chunks, chunks)
        return lax.rem(lax.div(kv, pair) + shift, chunks) * pair

    def forward_chunk(c):
        base = base_of(c)
        for i in range(pair):
            @pl.when(base + i != kv)
            def _():
                forward(gcomp, "g", base + i)

    pl.semaphore_wait(barrier, n_kv - 1 + n_tp - 1)
    peers = [
        base_of(jnp.int32(c)) + lax.rem(lax.rem(kv, pair) + i, pair)
        for c in range(chunks)
        for i in range(pair)
        if c + 1 < chunks or i > 0
    ]
    for d, peer in enumerate(peers):
        gather_copy(gcomp, "g", kv, peer, d).start()
    for d, peer in enumerate(peers):
        gather_copy(gkeys, "k", kv, peer, d).start()

    r["piece_keys"][:, 0:lat] = latent[0:rows]
    r["piece_keys"][:, lat:] = rotary[0:rows, 0:rot]
    r["decode_keys"][:, 0:lat] = latent[rows : rows + decodes]
    r["decode_keys"][:, lat:] = rotary[rows : rows + decodes, 0:rot]

    local["nope"].wait()
    local["rope"].wait()
    local["key_up"].wait()

    def make_queries(comp_rows, cosine, sine, q_ref):
        t = comp_rows.shape[0]
        qn = dot(comp_rows, r["nope"][...]).astype(BF16)
        qr = dot(comp_rows, r["rope"][...])
        width = qr.shape[1]
        reps = width // cosine.shape[1]
        cosine = jnp.concatenate([cosine] * reps, axis=1)
        sine = jnp.concatenate([sine] * reps, axis=1)
        qr = qr * cosine + swap_halves(qr, rot) * sine
        for h in range(heads):
            q_ref[h * t : (h + 1) * t, 0:lat] = dot(
                qn[:, h * nope_w : (h + 1) * nope_w], r["key_up"][h]
            ).astype(BF16)
            shift = (width - h * rot) % width
            part = pltpu.roll(qr, shift, 1) if shift else qr
            q_ref[h * t : (h + 1) * t, lat:] = part[:, 0:rot].astype(BF16)

    qo = r["qo"]
    make_queries(comp, tab[0], tab[1], qo)
    dq = jnp.concatenate([qo[h * total + rows : (h + 1) * total, :] for h in range(heads)], axis=0)
    drows = heads * extra

    local["dcache"].wait()
    dkeys_lat = latent[rows:total].astype(F32)
    dkeys_rot = rotary[rows:total, 0:rot].astype(F32)
    tiled_lat = jnp.concatenate([dkeys_lat] * heads, axis=0)
    tiled_rot = jnp.concatenate([dkeys_rot] * heads, axis=0)
    self_score = (
        jnp.sum(dq[:, 0:lat].astype(F32) * tiled_lat, axis=-1, keepdims=True)
        + jnp.sum(dq[:, lat:].astype(F32) * tiled_rot, axis=-1, keepdims=True)
    ) * scale
    row_of = lax.rem(lax.broadcasted_iota(jnp.int32, (drows, lat), 0), extra)
    dlat = jnp.zeros((drows, lat), F32)
    slots = r["dcache"].shape[2]
    for b in range(decodes):
        s = dot(dq, r["dcache"][b])
        live = lanes((drows, slots)) < r["lengths"][b]
        s = jnp.where(live, s * scale, NEG_FILL)
        m = jnp.maximum(jnp.max(s, axis=-1, keepdims=True), self_score)
        w = jnp.where(live, jnp.exp(s - m), 0.0)
        w_self = jnp.exp(self_score - m)
        norm = jnp.sum(w, axis=-1, keepdims=True) + w_self
        v = dot_t(w.astype(BF16), r["dcache"][b, 0:lat, :])
        v = (v + w_self.astype(BF16).astype(F32) * tiled_lat) / norm
        dlat = jnp.where(row_of == b, v, dlat)
    forward_chunk(jnp.int32(0))
    local["value_up"].wait()
    ho = r["ho"]
    for h in range(heads):
        ho[rows:total, h * vdim : (h + 1) * vdim] = dot_wide(
            dlat[h * extra : (h + 1) * extra], r["value_up"][h]
        ).astype(BF16)

    local["pcache"].wait()
    sendv, recvv = r["sendv"], r["recvv"]
    chunk = pair * rows
    qc = r["qc"]

    def value_copy(mine, peer):
        return pltpu.make_async_remote_copy(
            src_ref=sendv.at[peer], dst_ref=recvv.at[mine],
            send_sem=r["v_send"].at[peer], recv_sem=r["v_recv"].at[mine],
            device_id={"kv": peer}, device_id_type=MESH,
        )

    stat_lane = lanes((rows, 128))

    def stats(m, norm, t, start):
        out = jnp.zeros((rows, 128), F32)
        for h in range(heads):
            at = h * t + start
            out = jnp.where(stat_lane == h, m[at : at + rows], out)
            out = jnp.where(stat_lane == heads + h, norm[at : at + rows], out)
        return out

    def chunk_step(c, carry):
        base = base_of(c)

        @pl.when(c + 1 < chunks)
        def _():
            forward_chunk(c + 1)

        @pl.when(c + 1 == chunks)
        def _():
            for d in range(1, n_kv):
                forward(gkeys, "k", lax.rem(kv + d, n_kv))

        for i in range(pair):
            @pl.when(base + i != kv)
            def _():
                forwarded(gcomp, "g", base + i)
        at = pl.ds(pl.multiple_of(base * rows, chunk), chunk)
        comp_rows = gcomp[pl.ds(base, pair)].reshape(chunk, qrank)
        make_queries(comp_rows, r["cos"][at, :], r["sin"][at, :], qc)
        s = dot(qc[...], r["pcache"][...]) * scale
        m = jnp.max(s, axis=-1, keepdims=True)
        w = jnp.exp(s - m)
        norm = jnp.sum(w, axis=-1, keepdims=True)
        v = dot_t(w.astype(BF16), r["pcache"][0:lat, :]).astype(BF16)
        for h in range(heads):
            pv = dot(v[h * chunk : (h + 1) * chunk], r["value_up"][h]).astype(BF16)
            for i in range(pair):
                sendv[base + i, :, h * vdim : (h + 1) * vdim] = pv[i * rows : (i + 1) * rows]
        for i in range(pair):
            st = stats(m, norm, chunk, i * rows)
            high = st.astype(BF16).astype(F32)
            mid = (st - high).astype(BF16).astype(F32)
            low = (st - high) - mid
            packed = high + pltpu.roll(mid, 2 * heads, 1) + pltpu.roll(low, 4 * heads, 1)
            sendv[base + i, :, heads * vdim :] = packed.astype(BF16)
        for i in range(pair):
            @pl.when(base + i != kv)
            def _():
                value_copy(kv, base + i).start()
        return carry

    lax.fori_loop(0, n_kv // pair, chunk_step, 0)

    own_q = jnp.concatenate([qo[h * total : h * total + rows, :] for h in range(heads)], axis=0)
    for d in range(1, n_kv):
        forwarded(gkeys, "k", lax.rem(kv + d, n_kv))
    every = gkeys[...].reshape(piece_total, gkeys.shape[2])
    key_lat = every[:, 0:lat]
    s = dot_t(own_q[:, 0:lat], key_lat) + dot_t(own_q[:, lat:], every[:, lat : lat + rot])
    row = lax.rem(lax.broadcasted_iota(jnp.int32, s.shape, 0), rows) + kv * rows
    causal = lanes(s.shape) <= row
    s = jnp.where(causal, s * scale, NEG_FILL)
    m = jnp.max(s, axis=-1, keepdims=True)
    w = jnp.where(causal, jnp.exp(s - m), 0.0)
    norm = jnp.sum(w, axis=-1, keepdims=True)
    own_v = dot(w.astype(BF16), key_lat)
    own_stats = stats(m, norm, rows, 0)
    own_p = [dot_wide(own_v[h * rows : (h + 1) * rows], r["value_up"][h]) for h in range(heads)]

    recvv[kv] = sendv[kv]
    for d in range(1, n_kv):
        peer = lax.rem(kv + n_kv - d, n_kv)
        value_copy(peer, kv).wait_recv()
    joint = own_stats
    received = []
    for j in range(n_kv):
        st = recvv[j, :, heads * vdim :].astype(F32)
        st = st + pltpu.roll(st, 128 - 2 * heads, 1) + pltpu.roll(st, 128 - 4 * heads, 1)
        received.append(jnp.where(stat_lane < 2 * heads, st, 0.0))
        joint = jnp.maximum(joint, received[j])
    factor = jnp.exp(own_stats - joint)
    bottom = pltpu.roll(own_stats, 128 - heads, 1) * factor
    top = [own_p[h] * factor[:, h : h + 1] for h in range(heads)]
    for j in range(n_kv):
        st = received[j]
        factor = jnp.exp(st - joint)
        bottom = bottom + pltpu.roll(st, 128 - heads, 1) * factor
        for h in range(heads):
            top[h] = top[h] + recvv[j, :, h * vdim : (h + 1) * vdim].astype(F32) * factor[:, h : h + 1]
    for h in range(heads):
        ho[0:rows, h * vdim : (h + 1) * vdim] = (top[h] / bottom[:, h : h + 1]).astype(BF16)

    local["out_w"].wait()
    local["out_gain"].wait()
    mixs, mixr, sqs, sqr = r["mixs"], r["mixr"], r["sqs"], r["sqr"]
    cols = mixs.shape[2]

    def mix_copy(mine, peer):
        return pltpu.make_async_remote_copy(
            src_ref=mixs.at[peer], dst_ref=mixr.at[mine],
            send_sem=r["m_send"].at[peer], recv_sem=r["m_recv"].at[mine],
            device_id={"tp": peer}, device_id_type=MESH,
        )

    def square_copy(mine, peer):
        return pltpu.make_async_remote_copy(
            src_ref=sqs, dst_ref=sqr.at[mine],
            send_sem=r["q_send"].at[peer], recv_sem=r["q_recv"].at[mine],
            device_id={"tp": peer}, device_id_type=MESH,
        )

    head_out = ho[...]
    for d in range(1, n_tp):
        peer = lax.rem(tp + d, n_tp)
        at = pl.ds(pl.multiple_of(peer * cols, 128), cols)
        mixs[peer] = dot(head_out, r["out_w"][:, at]).astype(BF16)
        mix_copy(tp, peer).start()
    mix = dot(head_out, r["out_w"][:, pl.ds(pl.multiple_of(tp * cols, 128), cols)])
    for d in range(1, n_tp):
        peer = lax.rem(tp + n_tp - d, n_tp)
        mix_copy(peer, tp).wait_recv()
        mix = mix + mixr[peer].astype(F32)
    squares = jnp.sum(mix * mix, axis=-1, keepdims=True)
    diagonal = lax.broadcasted_iota(jnp.int32, (total, 128), 0) == lanes((total, 128))
    sqs[...] = jnp.broadcast_to(
        jnp.sum(jnp.where(diagonal, squares, 0.0), axis=0, keepdims=True), sqs.shape
    )
    for d in range(1, n_tp):
        square_copy(tp, lax.rem(tp + d, n_tp)).start()
    square_row = sqs[0:1, :]
    for d in range(1, n_tp):
        peer = lax.rem(tp + n_tp - d, n_tp)
        square_copy(peer, tp).wait_recv()
        square_row = square_row + sqr[peer, 0:1, :]
    squares = jnp.sum(jnp.where(diagonal, square_row, 0.0), axis=1, keepdims=True)
    result = mix * lax.rsqrt(squares / (cols * n_tp) + EPSILON) * r["out_gain"][...]
    r["piece_out"][...] = result[0:rows]
    r["decode_out"][...] = result[rows : rows + decodes]

    for d, peer in enumerate(peers):
        gather_copy(gcomp, "g", kv, peer, d).wait_send()
        gather_copy(gkeys, "k", kv, peer, d).wait_send()
        if share == 2:
            forward_copy(gcomp, "gf", peer, mine).wait_send()
            forward_copy(gkeys, "kf", peer, mine).wait_send()
        value_copy(kv, peer).wait_send()
    for d in range(1, n_tp):
        peer = lax.rem(tp + d, n_tp)
        mix_copy(tp, peer).wait_send()
        square_copy(tp, peer).wait_send()


def finish(*refs):
    count = len(refs) // 2
    for i in range(count):
        refs[count + i][...] = refs[i][...]


def shards(
    n_kv, n_tp,
    piece_tokens, decode_tokens, decode_lengths, prompt_cache, decode_cache, input_gain,
    query_down, query_gain, query_nope_weight, query_rope_weight, latent_weight, latent_gain,
    rotary_weight, key_up, value_up, out_weight, out_gain,
):
    rows, model = piece_tokens.shape
    decodes = decode_tokens.shape[0]
    extra = -(-decodes // 16) * 16
    total = rows + extra
    heads = key_up.shape[0]
    lat = latent_gain.shape[0]
    qrank = query_gain.shape[0]
    rot = rotary_weight.shape[1]
    pair = 2 if n_kv % 2 == 0 else 1
    wide = -(-rot // 128) * 128
    cols = out_gain.shape[0]

    args = {
        "lengths": decode_lengths,
        "piece": piece_tokens, "decode": decode_tokens, "input_gain": input_gain[None],
        "down": query_down, "query_gain": query_gain[None], "latent": latent_weight,
        "latent_gain": latent_gain[None], "rotary": rotary_weight.T,
        "nope": query_nope_weight, "rope": query_rope_weight, "key_up": key_up,
        "dcache": decode_cache.transpose(0, 2, 1), "pcache": prompt_cache.T, "value_up": value_up,
        "out_w": out_weight, "out_gain": out_gain[None],
    }
    outs = {
        "piece_out": ((rows, cols), F32), "decode_out": ((decodes, cols), F32),
        "piece_keys": ((rows, lat + rot), BF16), "decode_keys": ((decodes, lat + rot), BF16),
    }
    width = lat + rot
    vdim = value_up.shape[2]
    scratch = {k: pltpu.VMEM(v.shape, v.dtype) for k, v in args.items() if k != "lengths"}
    scratch |= {
        "tok": pltpu.VMEM((total, model), F32),
        "cos": pltpu.VMEM((rows * n_kv + extra, 128), F32),
        "sin": pltpu.VMEM((rows * n_kv + extra, 128), F32),
        "rk": pltpu.VMEM((total, 128), F32),
        "tab": pltpu.VMEM((2, total, 128), F32),
        "gcomp": pltpu.VMEM((n_kv, rows, qrank), BF16),
        "gkeys": pltpu.VMEM((n_kv, rows, lat + wide), BF16),
        "qo": pltpu.VMEM((heads * total, width), BF16),
        "qc": pltpu.VMEM((heads * pair * rows, width), BF16),
        "ho": pltpu.VMEM((total, heads * vdim), BF16),
        "sendv": pltpu.VMEM((n_kv, rows, heads * vdim + 128), BF16),
        "recvv": pltpu.VMEM((n_kv, rows, heads * vdim + 128), BF16),
        "mixs": pltpu.VMEM((n_tp, total, cols), BF16),
        "mixr": pltpu.VMEM((n_tp, total, cols), BF16),
        "sqs": pltpu.VMEM((8, 128), F32),
        "sqr": pltpu.VMEM((n_tp, 8, 128), F32),
        "load_sem": pltpu.SemaphoreType.DMA((len(args) - 1,)),
    }
    for k in ("g", "k", "gf", "kf", "v"):
        scratch[k + "_send"] = pltpu.SemaphoreType.DMA((n_kv,))
        scratch[k + "_recv"] = pltpu.SemaphoreType.DMA((n_kv,))
    for k in ("m", "q"):
        scratch[k + "_send"] = pltpu.SemaphoreType.DMA((n_tp,))
        scratch[k + "_recv"] = pltpu.SemaphoreType.DMA((n_tp,))
    names = [k if k == "lengths" else k + "_hbm" for k in args] + list(outs) + list(scratch)
    results = pl.pallas_call(
        functools.partial(kernel, n_kv, n_tp, pair, names),
        out_shape=[jax.ShapeDtypeStruct(*v) for v in outs.values()],
        in_specs=[
            pl.BlockSpec(memory_space=pltpu.SMEM if k == "lengths" else pl.ANY) for k in args
        ],
        out_specs=[pl.BlockSpec(memory_space=pltpu.VMEM) for _ in outs],
        scratch_shapes=list(scratch.values()),
        compiler_params=pltpu.CompilerParams(
            collective_id=0, has_side_effects=True, vmem_limit_bytes=60000 * 1024
        ),
    )(*args.values())
    return pl.pallas_call(
        finish,
        out_shape=[jax.ShapeDtypeStruct(*v) for v in outs.values()],
        in_specs=[pl.BlockSpec(memory_space=pltpu.VMEM) for _ in outs],
        out_specs=[pl.BlockSpec(memory_space=pltpu.VMEM) for _ in outs],
    )(*results)


def solution(mesh):
    in_specs = (
        P("kv", None), P("kv", None), P("kv"), P("kv", None), P("kv", None, None), P(), P(), P(),
        P(None, "tp"), P(None, "tp"), P(), P(), P(), P("tp", None, None), P("tp", None, None),
        P("tp", None), P("tp"),
    )
    out_specs = (P("kv", "tp"), P("kv", "tp"), P("kv", None), P("kv", None))
    body = functools.partial(shards, mesh.shape["kv"], mesh.shape["tp"])
    return jax.shard_map(
        body, mesh=mesh, in_specs=in_specs, out_specs=out_specs, check_vma=False
    )
```
